512 devices in a mesh: grp: 2 (over y), fs: 32 (over z), tp: 8 (over x, core).
Axes of the slice: x: 4, y: 2, z: 32, core: 2. Of those that a mesh axis runs over, the one named last changes fastest.
The devices are a block of a 4x8x32 slice.
Arguments:
- tokens: bfloat16 [20480, 2048], P(('grp', 'fs', 'tp')), parts along dimension 0, may hold values from -6 to 6
- mix_gain: bfloat16 [2048], replicated, may hold values from 0.099609375 to 1.8984375
- val_weight: bfloat16 [2048, 1024], P('fs', 'tp'), may hold values from -4 to 4
- gate_weight: bfloat16 [2048, 1024], P('fs', 'tp'), may hold values from -0.125 to 0.125
- conv_taps: bfloat16 [31, 1024], replicated, may hold values from -1 to 1
- chan_gain: bfloat16 [1024], replicated, may hold values from 0.099609375 to 1.8984375
- out_weight: bfloat16 [1024, 2048], P('tp', 'fs'), may hold values from -0.1875 to 0.1875
- mix_post_gain: bfloat16 [2048], replicated, may hold values from 0.099609375 to 1.8984375
- ffn_gain: bfloat16 [2048], replicated, may hold values from 0.099609375 to 1.8984375
- up_gate_weight: bfloat16 [2048, 5120], P('fs', 'tp'), may hold values from -0.125 to 0.125
- up_val_weight: bfloat16 [2048, 5120], P('fs', 'tp'), may hold values from -0.125 to 0.125
- ffn_taps: bfloat16 [2, 3, 5120], replicated, may hold values from -3.5 to 3.5
- down_weight: bfloat16 [5120, 2048], P('tp', 'fs'), may hold values from -0.078125 to 0.078125
- ffn_post_gain: bfloat16 [2048], replicated, may hold values from 0.099609375 to 1.8984375
Outputs:
- layer_out: bfloat16 [20480, 2048], P(('grp', 'fs', 'tp')), parts along dimension 0
The draws below stay inside these ranges and needn't reach their ends.
There are 2 independent parts, one for each index of `grp`. The reference program is written for one: setup_inputs(seed, part) draws one part's arguments, and reference() takes and returns one part's arrays. A program takes and returns all parts, laid end to end along the dimension named above; an argument that names none is the same for every part. Nothing has to cross between parts.
All inputs are finite; a program needn't handle non-finite values.
Results may differ from the reference program's by a relative error of at most 0.019.
Values may be sent and summed in bfloat16 or wider, within the bound.
A program may use at most 64 MiB of HBM per device.

```python
import jax
import jax.numpy as jnp
from jax import lax

D = 2048
CH = 1024
FF = 5120
CONV_TAPS = 31
FFN_TAPS = 3
LEN = 64
TOKENS = 10240
N_TP = 8


def draw_val_weight(key, part):
    base_key, rough_key = jax.random.split(key, 2)
    base_draw = jax.random.normal(base_key, (D, CH), jnp.float32) * D ** (-0.5)
    roughness = jnp.exp(jax.random.uniform(rough_key, (CH,), jnp.float32, -0.7, 0.7))
    position = jnp.arange(CH, dtype=jnp.float32) / CH
    drawn_values = base_draw * 4.0 ** position * roughness
    return jnp.clip(drawn_values, -4.0, 4.0).astype(jnp.bfloat16)


def shard_levels(rng, dims, pieces, smallest, top_value):
    level = 1.0
    for dim, shards_of in pieces:
        steps = jax.random.uniform(jax.random.fold_in(jax.random.fold_in(rng, 6), dim), (shards_of,), jnp.float32, smallest / len(pieces), top_value / len(pieces))
        level = level * jnp.repeat(jnp.exp(steps), dims[dim] // shards_of).reshape((-1,) + (1,) * (len(dims) - 1 - dim))
    return level


def gaussian(rng, shape, scale, most, cuts=(), held_as=jnp.bfloat16):
    values = jax.random.normal(rng, shape, jnp.float32) * scale
    if len(cuts) > 0:
        values = shard_levels(rng, shape, cuts, -0.22, 0.18) * values
    return jnp.clip(values, min=-most, max=most).astype(held_as)


def setup_inputs(seed: int = 0, part: int = 0) -> dict:
    splits = jax.random.split(jax.random.key(seed), 15)
    part_splits = jax.random.split(jax.random.fold_in(splits[14], part), 15)
    return {
        "tokens": gaussian(part_splits[0], (TOKENS, D), 1.0, 6.0, ((0, 256),)),
        "mix_gain": jnp.clip(1.0 + 0.18 * jax.random.normal(splits[1], (D,), jnp.float32), 0.099609375, 1.8984375).astype(jnp.bfloat16),
        "val_weight": draw_val_weight(jax.random.fold_in(splits[14], 71), part),
        "gate_weight": gaussian(splits[3], (D, CH), D ** -0.5, 0.125, ((0, 32), (1, 8))),
        "conv_taps": gaussian(splits[4], (CONV_TAPS, CH), CONV_TAPS ** -0.5, 1.0),
        "chan_gain": jnp.clip(1.0 + 0.18 * jax.random.normal(splits[5], (CH,), jnp.float32), 0.099609375, 1.8984375).astype(jnp.bfloat16),
        "out_weight": gaussian(splits[6], (CH, D), CH ** -0.5, 0.1875, ((0, 8), (1, 32))),
        "mix_post_gain": jnp.clip(1.0 + 0.18 * jax.random.normal(splits[7], (D,), jnp.float32), 0.099609375, 1.8984375).astype(jnp.bfloat16),
        "ffn_gain": jnp.clip(1.0 + 0.18 * jax.random.normal(splits[8], (D,), jnp.float32), 0.099609375, 1.8984375).astype(jnp.bfloat16),
        "up_gate_weight": gaussian(splits[9], (D, FF), D ** -0.5, 0.125, ((0, 32), (1, 8))),
        "up_val_weight": gaussian(splits[10], (D, FF), D ** -0.5, 0.125, ((0, 32), (1, 8))),
        "ffn_taps": gaussian(splits[11], (2, FFN_TAPS, FF), FFN_TAPS ** -0.5, 3.5),
        "down_weight": gaussian(splits[12], (FF, D), FF ** -0.5, 0.078125, ((0, 8), (1, 32))),
        "ffn_post_gain": jnp.clip(1.0 + 0.18 * jax.random.normal(splits[13], (D,), jnp.float32), 0.099609375, 1.8984375).astype(jnp.bfloat16),
    }


norm_epsilon = 1e-06
chan_epsilon = 1e-05

def rms_scale(values, gain):
    inverse = lax.rsqrt(lax.optimization_barrier(jnp.mean(values * values, axis=-1, keepdims=True)) + norm_epsilon)
    return values * inverse * gain.astype(jnp.float32)

def depthwise(signal, tap_table):
    taps_count = tap_table.shape[0]
    channels = signal.shape[1]
    shaped = signal.astype(jnp.float32).reshape(signal.shape[0] // LEN, LEN, channels)
    padded = jnp.pad(shaped, ((0, 0), (taps_count - 1, 0), (0, 0)))
    tap_values = tap_table.astype(jnp.float32)
    result = jnp.zeros(shaped.shape, jnp.float32)
    for offset in range(taps_count):
        result = result + padded[:, offset:offset + LEN, :] * tap_values[offset]
    return result.reshape(signal.shape[0], channels)

def grouped_sum(left, weight):
    group_width = left.shape[1] // N_TP

    def step(running, group_index):
        columns = lax.dynamic_slice_in_dim(left, group_index * group_width, group_width, 1)
        row_block = lax.dynamic_slice_in_dim(weight, group_index * group_width, group_width, 0)
        partial_value = jnp.dot(columns, row_block, preferred_element_type=jnp.float32).astype(jnp.bfloat16)
        partial_value = lax.optimization_barrier(partial_value)
        return (running + partial_value.astype(jnp.float32), None)
    start_sum = jnp.zeros((left.shape[0], weight.shape[1]), jnp.float32)
    running, _ = lax.scan(step, start_sum, jnp.arange(N_TP, dtype=jnp.int32))
    return running

def reference(tokens, mix_gain, val_weight, gate_weight, conv_taps, chan_gain, out_weight, mix_post_gain, ffn_gain, up_gate_weight, up_val_weight, ffn_taps, down_weight, ffn_post_gain):
    normed = rms_scale(tokens.astype(jnp.float32), mix_gain).astype(jnp.bfloat16)
    values = jnp.dot(normed, val_weight, preferred_element_type=jnp.float32)
    gate_sums = jnp.dot(normed, gate_weight, preferred_element_type=jnp.float32)
    glu_out = (values * jax.nn.sigmoid(gate_sums)).astype(jnp.bfloat16)
    conv_out = depthwise(glu_out, conv_taps)
    chan_mean = lax.optimization_barrier(jnp.mean(conv_out, axis=-1, keepdims=True))
    chan_var = lax.optimization_barrier(jnp.mean(conv_out * conv_out, axis=-1, keepdims=True)) - chan_mean * chan_mean
    scaled = (conv_out - chan_mean) * lax.rsqrt(chan_var + chan_epsilon) * chan_gain.astype(jnp.float32)
    activated = jax.nn.silu(scaled).astype(jnp.bfloat16)
    mixed_sum = grouped_sum(activated, out_weight)
    residual = (tokens.astype(jnp.float32) + rms_scale(mixed_sum, mix_post_gain)).astype(jnp.bfloat16)
    normed_ffn = rms_scale(residual.astype(jnp.float32), ffn_gain).astype(jnp.bfloat16)
    up_gate = jnp.dot(normed_ffn, up_gate_weight, preferred_element_type=jnp.float32).astype(jnp.bfloat16)
    up_val = jnp.dot(normed_ffn, up_val_weight, preferred_element_type=jnp.float32).astype(jnp.bfloat16)
    gate_conv = depthwise(up_gate, ffn_taps[0])
    val_conv = depthwise(up_val, ffn_taps[1])
    hidden = (jax.nn.gelu(gate_conv, approximate=True) * val_conv).astype(jnp.bfloat16)
    ffn_sum = grouped_sum(hidden, down_weight)
    return (residual.astype(jnp.float32) + rms_scale(ffn_sum, ffn_post_gain)).astype(jnp.bfloat16)
```

```python
import functools

import jax
import jax.numpy as jnp
from jax import lax
from jax.experimental import pallas as pl
from jax.experimental.pallas import tpu as pltpu
from jax.sharding import PartitionSpec as P

LEN = 64
MESH = pl.DeviceIdType.MESH
F32 = jnp.float32
BF16 = jnp.bfloat16
NT = (((1,), (1,)), ((), ()))

norm_epsilon = 1e-06
chan_epsilon = 1e-05

LANES = 128
PAIR = 2 * LANES
PAD_ROWS = 32
FPAD = 8


class Ring:
    def __init__(self, n, me, block, streams, offsets, send_sem, recv_sem):
        self.n, self.me, self.block = n, me, block
        self.streams, self.offsets = streams, offsets
        self.send_sem, self.recv_sem = send_sem, recv_sem
        self.steps = (n // 2, (n - 1) - n // 2)
        self.peers = (lax.rem(me + 1, n), lax.rem(me + n - 1, n))
        self.at = 0
        self.last = max(offsets) + self.steps[0]

    def copy(self, j, way, owner, step):
        ref = self.streams[j](owner)
        return pltpu.make_async_remote_copy(
            src_ref=ref,
            dst_ref=ref,
            send_sem=self.send_sem.at[j, way],
            recv_sem=self.recv_sem.at[j, way, step],
            device_id={"fs": self.peers[way]},
            device_id_type=MESH,
        )

    def owner(self, way, step):
        shift = (self.n - step) if way == 0 else step
        return lax.rem(self.me + shift, self.n)

    def arrived(self, j, way, step):
        self.copy(j, way, self.owner(way, step + 1), step).wait_recv()

    def slot(self, k, active):
        for j, first in active:
            for way in (0, 1):
                step = k - self.offsets[j]
                if first:
                    if self.steps[way] > 0:
                        self.copy(j, way, self.me, 0).start()
                    continue

                def go(j=j, way=way, step=step):
                    self.arrived(j, way, step - 1)
                    self.copy(j, way, self.owner(way, step), step).start()

                if way == 0 or isinstance(step, int):
                    if step < self.steps[way] if isinstance(step, int) else True:
                        go()
                else:
                    pl.when(step < self.steps[way])(go)

    def active(self, k):
        return tuple(
            (j, k == off)
            for j, off in enumerate(self.offsets)
            if off <= k < off + self.steps[0]
        )

    def short(self, k):
        return tuple(k - off >= self.steps[1] for off in self.offsets)

    def pump_to(self, upto):
        upto = min(upto, self.last)
        while self.at < upto:
            key = (self.active(self.at), self.short(self.at))
            end = self.at
            while end < upto and (self.active(end), self.short(end)) == key:
                end += 1
            steady = end - self.at > 1 and not any(f for _, f in key[0])
            if steady and not any(key[1][j] for j, _ in key[0]):
                lax.fori_loop(
                    self.at, end, lambda k, z, key=key: (self.slot_loop(k, key[0]), z)[1], 0
                )
                self.at = end
            else:
                self.slot(self.at, self.active(self.at))
                self.at += 1

    def slot_loop(self, k, active):
        for j, _ in active:
            for way in (0, 1):
                step = k - self.offsets[j]
                self.arrived(j, way, step - 1)
                self.copy(j, way, self.owner(way, step), step).start()

    def finish(self, js):
        self.pump_to(max(self.offsets[j] + self.steps[0] for j in js))
        for j in js:
            for way in (0, 1):
                if self.steps[way] > 0:
                    self.arrived(j, way, self.steps[way] - 1)

    def drain(self, wholes):
        for j, whole in enumerate(wholes):
            for way in (0, 1):
                if self.steps[way] > 0:
                    ref = whole(self.steps[way])
                    pltpu.make_async_copy(ref, ref, self.send_sem.at[j, way]).wait()


def layer_kernel(
    n,
    tp,
    tokens,
    mix_gain,
    val_h,
    gate_h,
    conv_taps,
    chan_gain,
    out_w,
    mix_post_gain,
    ffn_gain,
    up_gate_h,
    up_val_h,
    ffn_taps,
    down_w,
    ffn_post_gain,
    out,
    vg,
    outt,
    up,
    downt,
    xg,
    lhs,
    prod,
    din,
    psum,
    opp,
    near,
    comb,
    fin,
    got,
    cbuf,
    conv,
    stats,
    resid,
    fbuf,
    hidden,
    load_sem,
    zsend,
    zrecv,
    xsend,
    xrecv,
    ssend,
    srecv,
):
    rows, width = tokens.shape
    half, quarter = width // 2, width // 4
    block = width // n
    group_rows = rows * tp
    chip_rows = 2 * rows
    chips = tp // 2
    pieces = up_gate_h.shape[1] // LANES
    f = lax.axis_index("fs")
    t = lax.axis_index("tp")
    x, c = t // 2, lax.rem(t, 2)
    partner = t + 1 - 2 * c
    xr, xl, xo = (lax.rem(x + s, chips) for s in (1, chips - 1, 2))
    tr, tl, to = (2 * v + c for v in (xr, xl, xo))
    odd = c == 1

    mine = pl.ds(pl.multiple_of(f * block, block), block)
    loads = [
        pltpu.make_async_copy(val_h, vg.at[mine, pl.ds(0, LANES)], load_sem.at[0]),
        pltpu.make_async_copy(gate_h, vg.at[mine, pl.ds(LANES, LANES)], load_sem.at[1]),
    ]
    for j in range(pieces):
        columns = pl.ds(j * LANES, LANES)
        loads.append(
            pltpu.make_async_copy(
                up_gate_h.at[:, columns], up.at[j, mine, pl.ds(0, LANES)], load_sem.at[2 + 2 * j]
            )
        )
        loads.append(
            pltpu.make_async_copy(
                up_val_h.at[:, columns], up.at[j, mine, pl.ds(LANES, LANES)], load_sem.at[3 + 2 * j]
            )
        )
    for load in loads:
        load.start()

    barrier = pltpu.get_barrier_semaphore()
    for z in (lax.rem(f + 1, n), lax.rem(f + n - 1, n)):
        pl.semaphore_signal(barrier, inc=1, device_id={"fs": z}, device_id_type=MESH)
    for d in range(1, tp):
        pl.semaphore_signal(
            barrier, inc=1, device_id={"tp": lax.rem(t + d, tp)}, device_id_type=MESH
        )

    eye = jnp.where(
        lax.broadcasted_iota(jnp.int32, (block, block), 0)
        == lax.broadcasted_iota(jnp.int32, (block, block), 1),
        1.0,
        0.0,
    ).astype(BF16)
    outt[mine, :] = lax.dot_general(eye, out_w[...], NT, preferred_element_type=F32).astype(BF16)
    downt[mine, :] = lax.dot_general(eye, down_w[...], NT, preferred_element_type=F32).astype(BF16)

    def zview(buffer, owner):
        return buffer.at[pl.ds(pl.multiple_of(owner * block, block), block), :]

    def down_view(part, owner):
        size = block // 2
        start = pl.multiple_of(owner * block + part * size, size)
        return downt.at[pl.ds(start, size), :]

    streams = [functools.partial(zview, vg), functools.partial(zview, outt)]
    streams += [functools.partial(zview, up.at[j]) for j in range(pieces)]
    streams += [functools.partial(down_view, part) for part in (0, 1)]
    steps = n // 2
    ups = list(range(2, 2 + pieces))
    downs = [2 + pieces, 3 + pieces]
    offsets = [0, 0] + [0 if j < 2 else steps for j in range(pieces)] + [2 * steps] * 2
    ring = Ring(n, f, block, streams, offsets, zsend, zrecv)

    def put_normed(u, left, right, gain):
        scale = lax.rsqrt(
            (
                jnp.sum(left * left, axis=1, keepdims=True)
                + jnp.sum(right * right, axis=1, keepdims=True)
            )
            / width
            + norm_epsilon
        )
        pad = jnp.zeros((8, half), F32)
        for at, part in ((0, left), (half, right)):
            value = part * scale * gain[:, at : at + half].astype(F32)
            low = jnp.concatenate([value, pad], axis=0)
            high = jnp.concatenate([pad, value], axis=0)
            xg[u, t, :, at : at + half] = jnp.where(odd, high, low).astype(BF16)

    def x_copy(u, sem, src, dst, where):
        return pltpu.make_async_remote_copy(
            src_ref=src,
            dst_ref=dst,
            send_sem=xsend.at[u, sem],
            recv_sem=xrecv.at[u, sem],
            device_id={"tp": where},
            device_id_type=MESH,
        )

    first, second = pl.ds(0, half), pl.ds(half, half)

    def spread(u, slots):
        own, from_l, from_r = xg.at[u, t], xg.at[u, tl], xg.at[u, tr]
        opp_l, opp_r = xg.at[u, to, :, first], xg.at[u, to, :, second]
        sent = [
            x_copy(u, 1, own, own, tr),
            x_copy(u, 2, own, own, tl),
            x_copy(u, 0, own, own, partner),
        ]
        for copy in sent:
            copy.start()
        ring.pump_to(slots[0])
        more = []
        x_copy(u, 1, from_l, from_l, tr).wait_recv()
        more.append(x_copy(u, 3, from_l.at[:, first], from_l.at[:, first], tr))
        more.append(x_copy(u, 5, from_l, from_l, partner))
        more[0].start()
        x_copy(u, 2, from_r, from_r, tl).wait_recv()
        more.append(x_copy(u, 4, from_r.at[:, second], from_r.at[:, second], tl))
        more.append(x_copy(u, 6, from_r, from_r, partner))
        for copy in more[2:3] + more[1:2] + more[3:4]:
            copy.start()
        sent += more
        ring.pump_to(slots[1])
        x_copy(u, 3, opp_l, opp_l, tr).wait_recv()
        last = [x_copy(u, 7, opp_l, opp_l, partner)]
        last[0].start()
        x_copy(u, 4, opp_r, opp_r, tl).wait_recv()
        last.append(x_copy(u, 8, opp_r, opp_r, partner))
        last[1].start()
        sent += last
        ring.pump_to(slots[2])
        other = 1 - 2 * c
        for sem, ref in (
            (0, xg.at[u, partner]),
            (5, xg.at[u, tl + other]),
            (6, xg.at[u, tr + other]),
            (7, xg.at[u, to + other, :, first]),
            (8, xg.at[u, to + other, :, second]),
        ):
            x_copy(u, sem, ref, ref, partner).wait_recv()
        for chip in range(chips):
            a, b, base = xg.at[u, 2 * chip], xg.at[u, 2 * chip + 1], chip * chip_rows
            lhs[base : base + 32, :] = a[0:32, :]
            lhs[base + 32 : base + 48, :] = a[32:48, :] + b[0:16, :]
            lhs[base + 48 : base + 80, :] = b[16:48, :]
        return sent

    def chip_rows_at(v):
        return pl.ds(pl.multiple_of(v * chip_rows, 16), chip_rows)

    q0, q1 = pl.ds(0, quarter), pl.ds(quarter, quarter)

    def collect(u, slots):
        mine_h = pl.ds(pl.multiple_of(c * half, half), half)
        other_h = pl.ds(pl.multiple_of((1 - c) * half, half), half)
        sent = [x_copy(u, 9, prod.at[u, :, other_h], din.at[u], partner)]
        sent[0].start()
        ring.pump_to(slots[0])
        x_copy(u, 9, prod.at[u, :, other_h], din.at[u], partner).wait_recv()
        psum[u, :, :] = (
            prod[u, :, mine_h].astype(F32) + din[u, :, :].astype(F32)
        ).astype(BF16)
        plan = [
            (10, psum.at[u, chip_rows_at(xo), q0], opp.at[u, 0], tr),
            (11, psum.at[u, chip_rows_at(xo), q1], opp.at[u, 1], tl),
            (12, psum.at[u, chip_rows_at(xr), q1], near.at[u, 0, 1], tr),
            (13, psum.at[u, chip_rows_at(xl), q0], near.at[u, 1, 0], tl),
        ]
        for item in plan:
            copy = x_copy(u, *item)
            copy.start()
            sent.append(copy)
        ring.pump_to(slots[1])
        for way, sem, v, q, where in ((0, 10, xr, q0, tr), (1, 11, xl, q1, tl)):
            x_copy(u, sem, psum.at[u, chip_rows_at(xo), q], opp.at[u, way], where).wait_recv()
            comb[u, way, :, :] = (
                psum[u, chip_rows_at(v), q].astype(F32) + opp[u, way, :, :].astype(F32)
            ).astype(BF16)
            copy = x_copy(u, 14 + way, comb.at[u, way], near.at[u, way, way], where)
            copy.start()
            sent.append(copy)
        ring.pump_to(slots[2])
        for sem, way, part, where in ((12, 0, 1, tr), (13, 1, 0, tl), (14, 0, 0, tr), (15, 1, 1, tl)):
            x_copy(u, sem, comb.at[u, way], near.at[u, way, part], where).wait_recv()
        for part, q in ((0, q0), (1, q1)):
            fin[u, :, q] = (
                psum[u, chip_rows_at(x), q].astype(F32)
                + near[u, 0, part, :, :].astype(F32)
                + near[u, 1, part, :, :].astype(F32)
            )
        mine_r = pl.ds(pl.multiple_of(c * rows, 8), rows)
        other_r = pl.ds(pl.multiple_of((1 - c) * rows, 8), rows)
        copy = x_copy(u, 16, fin.at[u, other_r, :], got.at[u], partner)
        copy.start()
        sent.append(copy)
        ring.pump_to(slots[3])
        copy.wait_recv()
        here, there = fin[u, mine_r, :], got[u, :, :]
        return jnp.where(odd, there, here), jnp.where(odd, here, there), sent

    left = tokens[:, 0:half].astype(F32)
    right = tokens[:, half:width].astype(F32)
    put_normed(0, left, right, mix_gain)
    pl.semaphore_wait(barrier, tp + 1)
    for load in loads:
        load.wait()
    ring.pump_to(1)
    sent = spread(0, (2, 4, 5))

    ring.finish([0])
    both = jnp.dot(lhs[...], vg[...], preferred_element_type=F32)
    glu = (both[:, 0:LANES] * jax.nn.sigmoid(both[:, LANES:PAIR])).astype(BF16).astype(F32)
    segments = group_rows // LEN
    taps_n = conv_taps.shape[0]
    cbuf[:, 0:PAD_ROWS, :] = jnp.zeros((segments, PAD_ROWS, LANES), F32)
    for s in range(segments):
        cbuf[s, PAD_ROWS:, :] = glu[s * LEN : (s + 1) * LEN, :]
    my_ch = pl.ds(pl.multiple_of(t * LANES, LANES), LANES)
    taps = conv_taps[:, my_ch].astype(F32)

    def convolve(s, z):
        total = jnp.zeros((LEN, LANES), F32)
        for k in range(taps_n):
            at = PAD_ROWS - (taps_n - 1) + k
            total = total + cbuf[s, at : at + LEN, :] * taps[k : k + 1, :]
        conv[pl.ds(pl.multiple_of(s * LEN, LEN), LEN), :] = total
        return z

    lax.fori_loop(0, segments, convolve, 0)
    conv_out = conv[...]
    ones = jnp.ones((8, LANES), F32)
    high = lax.Precision.HIGHEST
    sums = lax.dot_general(ones, conv_out, NT, precision=high, preferred_element_type=F32)
    squares = lax.dot_general(
        ones, conv_out * conv_out, NT, precision=high, preferred_element_type=F32
    )
    pick = lax.broadcasted_iota(jnp.int32, (8, group_rows), 0) < 4
    stats[t, :, 0:group_rows] = jnp.where(pick, sums, squares)

    def stat_copy(d):
        return pltpu.make_async_remote_copy(
            src_ref=stats.at[t],
            dst_ref=stats.at[t],
            send_sem=ssend.at[d - 1],
            recv_sem=srecv.at[d - 1],
            device_id={"tp": lax.rem(t + d, tp)},
            device_id_type=MESH,
        )

    stat_copies = [stat_copy(d) for d in range(1, tp)]
    for copy in stat_copies:
        copy.start()
    ring.finish([1])
    for d in range(1, tp):
        source = lax.rem(t + tp - d, tp)
        pltpu.make_async_remote_copy(
            src_ref=stats.at[source],
            dst_ref=stats.at[source],
            send_sem=ssend.at[d - 1],
            recv_sem=srecv.at[d - 1],
            device_id={"tp": source},
            device_id_type=MESH,
        ).wait_recv()
    channels = chan_gain.shape[1]
    both_stats = jnp.sum(stats[:, :, 0:group_rows], axis=0) / channels
    flipped = jnp.transpose(
        jnp.concatenate([both_stats] + [jnp.zeros((8, group_rows), F32)] * 15, axis=0)
    )
    mean, square = flipped[:, 0:1], flipped[:, 4:5]
    scale = lax.rsqrt(square - mean * mean + chan_epsilon)
    normal = (conv_out - mean) * scale * chan_gain[:, my_ch].astype(F32)
    activated = (normal * jax.nn.sigmoid(normal)).astype(BF16)
    wide = min(512, width)
    for j in range(width // wide):
        prod[0, :, j * wide : (j + 1) * wide] = lax.dot_general(
            activated, outt[j * wide : (j + 1) * wide, :], NT, preferred_element_type=F32
        ).astype(BF16)

    base = ring.at
    left_sum, right_sum, more = collect(0, (base + 1, base + 2, base + 4, base + 5))
    sent += more

    def rms(a, b, gain):
        scale = lax.rsqrt(
            (jnp.sum(a * a, axis=1, keepdims=True) + jnp.sum(b * b, axis=1, keepdims=True)) / width
            + norm_epsilon
        )
        return (
            a * scale * gain[:, 0:half].astype(F32),
            b * scale * gain[:, half:width].astype(F32),
        )

    a, b = rms(left_sum, right_sum, mix_post_gain)
    res_a = (tokens[:, 0:half].astype(F32) + a).astype(BF16)
    res_b = (tokens[:, half:width].astype(F32) + b).astype(BF16)
    resid[:, 0:half] = res_a.astype(F32)
    resid[:, half:width] = res_b.astype(F32)
    put_normed(1, res_a.astype(F32), res_b.astype(F32), ffn_gain)
    base = ring.at
    sent += spread(1, (base + 1, base + 2, base + 3))

    fbuf[:, 0:FPAD, :] = jnp.zeros((segments, FPAD, PAIR), F32)
    ftaps_n = ffn_taps.shape[1]

    def feed(j):
        pair = jnp.dot(lhs[...], up[j], preferred_element_type=F32).astype(BF16).astype(F32)
        for s in range(segments):
            fbuf[s, FPAD:, :] = pair[s * LEN : (s + 1) * LEN, :]
        here = pl.ds(pl.multiple_of(t * (pieces * LANES) + j * LANES, LANES), LANES)
        gate_taps = ffn_taps[0, :, here].astype(F32)
        val_taps = ffn_taps[1, :, here].astype(F32)
        for s in range(segments):
            gate = jnp.zeros((LEN, LANES), F32)
            val = jnp.zeros((LEN, LANES), F32)
            for k in range(ftaps_n):
                at = FPAD - (ftaps_n - 1) + k
                gate = gate + fbuf[s, at : at + LEN, 0:LANES] * gate_taps[k : k + 1, :]
                val = val + fbuf[s, at : at + LEN, LANES:PAIR] * val_taps[k : k + 1, :]
            hidden[j, s * LEN : (s + 1) * LEN, :] = (
                jax.nn.gelu(gate, approximate=True) * val
            ).astype(BF16)

    early = [j for j in range(pieces) if offsets[2 + j] == 0]
    late = [j for j in range(pieces) if offsets[2 + j] > 0]
    ring.finish([2 + j for j in early])
    for j in early:
        feed(j)
        ring.pump_to(ring.at + 1)
    ring.finish([2 + j for j in late])
    for j in late:
        feed(j)
        ring.pump_to(ring.at + 2)
    ring.finish(downs)

    def contract(j, z):
        columns = pl.ds(pl.multiple_of(j * PAIR, PAIR), PAIR)
        units = jnp.concatenate([hidden[i] for i in range(pieces)], axis=1)
        prod[1, :, columns] = lax.dot_general(
            units, downt[columns, :], NT, preferred_element_type=F32
        ).astype(BF16)
        return z

    lax.fori_loop(0, width // PAIR, contract, 0)
    left_sum, right_sum, more = collect(1, (0, 0, 0, 0))
    sent += more
    a, b = rms(left_sum, right_sum, ffn_post_gain)
    out[:, 0:half] = (resid[:, 0:half] + a).astype(BF16)
    out[:, half:width] = (resid[:, half:width] + b).astype(BF16)

    for copy in sent + stat_copies:
        copy.wait_send()

    def whole_of(buffer, size, count):
        return buffer.at[pl.ds(0, count * size), :]

    wholes = [functools.partial(whole_of, vg, block), functools.partial(whole_of, outt, block)]
    wholes += [functools.partial(whole_of, up.at[j], block) for j in range(pieces)]
    wholes += [functools.partial(whole_of, downt, block // 2)] * 2
    ring.drain(wholes)


def shards(*args):
    (tokens, mix_gain, val_weight, _, conv_taps, chan_gain, out_weight) = args[:7]
    up_weight, down_weight = args[9], args[12]
    n, tp = lax.axis_size("fs"), lax.axis_size("tp")
    rows, width = tokens.shape
    block = width // n
    half, quarter = width // 2, width // 4
    group_rows, chip_rows = rows * tp, 2 * rows
    segments = group_rows // LEN
    pieces = up_weight.shape[1] // LANES
    streams = 4 + pieces
    steps = n // 2
    args = [a.reshape(1, -1) if a.ndim == 1 else a for a in args]
    vmem = pl.BlockSpec(memory_space=pltpu.VMEM)
    hbm = pl.BlockSpec(memory_space=pltpu.HBM)
    dma = pltpu.SemaphoreType.DMA
    return pl.pallas_call(
        functools.partial(layer_kernel, n, tp),
        out_shape=jax.ShapeDtypeStruct((rows, width), BF16),
        in_specs=[hbm if i in (2, 3, 9, 10) else vmem for i in range(len(args))],
        out_specs=vmem,
        scratch_shapes=[
            pltpu.VMEM((width, PAIR), BF16),
            pltpu.VMEM((width, LANES), BF16),
            pltpu.VMEM((pieces, width, PAIR), BF16),
            pltpu.VMEM((width, pieces * LANES), BF16),
            pltpu.VMEM((2, tp, rows + 8, width), BF16),
            pltpu.VMEM((group_rows, width), BF16),
            pltpu.VMEM((2, group_rows, width), BF16),
            pltpu.VMEM((2, group_rows, half), BF16),
            pltpu.VMEM((2, group_rows, half), BF16),
            pltpu.VMEM((2, 2, chip_rows, quarter), BF16),
            pltpu.VMEM((2, 2, 2, chip_rows, quarter), BF16),
            pltpu.VMEM((2, 2, chip_rows, quarter), BF16),
            pltpu.VMEM((2, chip_rows, half), F32),
            pltpu.VMEM((2, rows, half), F32),
            pltpu.VMEM((segments, PAD_ROWS + LEN, LANES), F32),
            pltpu.VMEM((group_rows, LANES), F32),
            pltpu.VMEM((tp, 8, pl.cdiv(group_rows, LANES) * LANES), F32),
            pltpu.VMEM((rows, width), F32),
            pltpu.VMEM((segments, FPAD + LEN, PAIR), F32),
            pltpu.VMEM((pieces, group_rows, LANES), BF16),
            dma((2 + 2 * pieces,)),
            dma((streams, 2)),
            dma((streams, 2, steps)),
            dma((2, 17)),
            dma((2, 17)),
            dma((tp - 1,)),
            dma((tp - 1,)),
        ],
        compiler_params=pltpu.CompilerParams(
            collective_id=0, has_side_effects=True, vmem_limit_bytes=60 * 1024 * 1024
        ),
    )(*args)


def solution(mesh):
    return jax.shard_map(
        shards,
        mesh=mesh,
        in_specs=(
            P(("grp", "fs", "tp"), None),
            P(),
            P("fs", "tp"),
            P("fs", "tp"),
            P(),
            P(),
            P("tp", "fs"),
            P(),
            P(),
            P("fs", "tp"),
            P("fs", "tp"),
            P(),
            P("tp", "fs"),
            P(),
        ),
        out_specs=P(("grp", "fs", "tp"), None),
        check_vma=False,
    )
```

```python
import functools

import jax
import jax.numpy as jnp
from jax import lax
from jax.experimental import pallas as pl
from jax.experimental.pallas import tpu as pltpu
from jax.sharding import PartitionSpec as P

LEN = 64
MESH = pl.DeviceIdType.MESH
F32 = jnp.float32
BF16 = jnp.bfloat16
NT = (((1,), (1,)), ((), ()))

norm_epsilon = 1e-06
chan_epsilon = 1e-05

LANES = 128
PAIR = 2 * LANES
PAD_ROWS = 32
LATE = 0
FPAD = 8


class Ring:
    def __init__(self, n, me, streams, offsets, shared, mate, sems):
        self.n, self.me = n, me
        self.streams, self.offsets, self.shared, self.mate = streams, offsets, shared, mate
        self.send_sem, self.recv_sem, self.ysend, self.yrecv = sems
        self.steps = (n // 2, (n - 1) - n // 2)
        self.peers = (lax.rem(me + 1, n), lax.rem(me + n - 1, n))
        self.at = 0
        self.last = max(offsets) + self.steps[0] + 1

    def copy(self, j, way, owner, step):
        ref = self.streams[j](owner)
        return pltpu.make_async_remote_copy(
            src_ref=ref,
            dst_ref=ref,
            send_sem=self.send_sem.at[j, way],
            recv_sem=self.recv_sem.at[j, way, step],
            device_id={"fs": self.peers[way]},
            device_id_type=MESH,
        )

    def across(self, j, owner):
        if j in self.shared:
            ref = self.streams[j](owner)
            pltpu.make_async_remote_copy(
                src_ref=ref,
                dst_ref=ref,
                send_sem=self.ysend.at[j],
                recv_sem=self.yrecv.at[j],
                device_id={"grp": self.mate},
                device_id_type=MESH,
            ).start()

    def owner(self, way, step):
        shift = (self.n - step) if way == 0 else step
        return lax.rem(self.me + shift, self.n)

    def step(self, j, way, step, forward):
        owner = self.owner(way, step)
        self.copy(j, way, owner, step - 1).wait_recv()
        if forward:
            self.copy(j, way, owner, step).start()
        self.across(j, owner)

    def slot(self, k):
        for j, off in enumerate(self.offsets):
            for way in (0, 1):
                step = k - off
                if step == 0:
                    if self.steps[way] > 0:
                        self.copy(j, way, self.me, 0).start()
                elif 0 < step <= self.steps[way]:
                    self.step(j, way, step, step < self.steps[way])

    def slot_loop(self, k, active):
        for j in active:
            for way in (0, 1):
                self.step(j, way, k - self.offsets[j], True)

    def kinds(self, k):
        passing, other = [], False
        for j, off in enumerate(self.offsets):
            step = k - off
            if 0 < step < self.steps[1]:
                passing.append(j)
            elif 0 <= step <= self.steps[0]:
                other = True
        return tuple(passing), other

    def pump_to(self, upto):
        upto = min(upto, self.last)
        while self.at < upto:
            kinds = self.kinds(self.at)
            end = self.at + 1
            while end < upto and not kinds[1] and self.kinds(end) == kinds:
                end += 1
            if end - self.at > 1:
                lax.fori_loop(
                    self.at, end, lambda k, z, on=kinds[0]: (self.slot_loop(k, on), z)[1], 0
                )
            else:
                self.slot(self.at)
            self.at = end

    def pump(self, count=1):
        self.pump_to(self.at + count)

    def finish(self, js):
        self.pump_to(max(self.offsets[j] for j in js) + self.steps[0] + 1)

    def handed(self, j, whole):
        pltpu.make_async_copy(whole, whole, self.yrecv.at[j]).wait()

    def drain(self, wholes):
        for j, whole in enumerate(wholes):
            for way in (0, 1):
                if self.steps[way] > 0:
                    ref = whole(self.steps[way])
                    pltpu.make_async_copy(ref, ref, self.send_sem.at[j, way]).wait()
            if j in self.shared:
                ref = whole(self.n - 1)
                pltpu.make_async_copy(ref, ref, self.ysend.at[j]).wait()


def layer_kernel(
    n,
    tp,
    tokens,
    mix_gain,
    val_h,
    gate_h,
    conv_taps,
    chan_gain,
    out_h,
    mix_post_gain,
    ffn_gain,
    up_gate_h,
    up_val_h,
    ffn_taps,
    down_h,
    ffn_post_gain,
    out,
    vg,
    outt,
    up,
    downt,
    xg,
    lhs,
    prod,
    din,
    psum,
    opp,
    near,
    comb,
    fin,
    got,
    cbuf,
    conv,
    stats,
    resid,
    fbuf,
    hidden,
    cgain,
    load_sem,
    zsend,
    zrecv,
    ysend,
    yrecv,
    xsend,
    xrecv,
    ssend,
    srecv,
):
    rows, width = tokens.shape
    half, quarter = width // 2, width // 4
    block = width // n
    group_rows = rows * tp
    chip_rows = 2 * rows
    chips = tp // 2
    pieces = up_gate_h.shape[1] // LANES
    f = lax.axis_index("fs")
    t = lax.axis_index("tp")
    x, c = t // 2, lax.rem(t, 2)
    partner = t + 1 - 2 * c
    xr, xl, xo = (lax.rem(x + s, chips) for s in (1, chips - 1, 2))
    tr, tl, to = (2 * v + c for v in (xr, xl, xo))
    odd = c == 1
    g = lax.axis_index("grp")
    side = lax.rem(g, 2)
    mate = g + 1 - 2 * side

    mine = pl.ds(pl.multiple_of(f * block, block), block)
    loads = [
        pltpu.make_async_copy(val_h, vg.at[mine, pl.ds(0, LANES)], load_sem.at[0]),
        pltpu.make_async_copy(gate_h, vg.at[mine, pl.ds(LANES, LANES)], load_sem.at[1]),
    ]
    for j in range(pieces):
        columns = pl.ds(j * LANES, LANES)
        loads.append(
            pltpu.make_async_copy(
                up_gate_h.at[:, columns], up.at[j, mine, pl.ds(0, LANES)], load_sem.at[2 + 2 * j]
            )
        )
        loads.append(
            pltpu.make_async_copy(
                up_val_h.at[:, columns], up.at[j, mine, pl.ds(LANES, LANES)], load_sem.at[3 + 2 * j]
            )
        )
    loads.append(pltpu.make_async_copy(out_h, outt.at[mine, :], load_sem.at[2 + 2 * pieces]))
    loads.append(pltpu.make_async_copy(down_h, downt.at[mine, :], load_sem.at[3 + 2 * pieces]))
    for load in loads:
        load.start()

    barrier = pltpu.get_barrier_semaphore()
    for z in (lax.rem(f + 1, n), lax.rem(f + n - 1, n)):
        pl.semaphore_signal(barrier, inc=1, device_id={"fs": z}, device_id_type=MESH)
    for d in range(1, tp):
        pl.semaphore_signal(
            barrier, inc=1, device_id={"tp": lax.rem(t + d, tp)}, device_id_type=MESH
        )

    pl.semaphore_signal(barrier, inc=1, device_id={"grp": mate}, device_id_type=MESH)

    def zview(buffer, owner):
        return buffer.at[pl.ds(pl.multiple_of(owner * block, block), block), :]

    def down_view(part, owner):
        size = block // 2
        start = pl.multiple_of(owner * block + part * size, size)
        return downt.at[pl.ds(start, size), :]

    share = pieces // 2
    own = [side * share + i for i in range(share)]
    far = [(1 - side) * share + i for i in range(share)]
    both_sides = list(range(2 * share, pieces))
    streams = [functools.partial(zview, vg), functools.partial(zview, outt)]
    streams += [functools.partial(zview, up.at[j]) for j in own]
    streams += [functools.partial(down_view, side)]
    streams += [functools.partial(zview, up.at[j]) for j in both_sides]
    own_at = list(range(2, 2 + share))
    down_at = 2 + share
    both_at = list(range(down_at + 1, len(streams)))
    offsets = [0, 0] + [0] * share + [min(LATE, n // 2)] * (1 + len(both_sides))
    ring = Ring(n, f, streams, offsets, own_at + [down_at], mate, (zsend, zrecv, ysend, yrecv))

    def put_normed(u, left, right, gain):
        scale = lax.rsqrt(
            (
                jnp.sum(left * left, axis=1, keepdims=True)
                + jnp.sum(right * right, axis=1, keepdims=True)
            )
            / width
            + norm_epsilon
        )
        pad = jnp.zeros((8, half), F32)
        for at, part in ((0, left), (half, right)):
            value = part * scale * gain[at : at + half].astype(F32).reshape(1, half)
            low = jnp.concatenate([value, pad], axis=0)
            high = jnp.concatenate([pad, value], axis=0)
            xg[u, t, :, at : at + half] = jnp.where(odd, high, low).astype(BF16)

    def x_copy(u, sem, src, dst, where):
        return pltpu.make_async_remote_copy(
            src_ref=src,
            dst_ref=dst,
            send_sem=xsend.at[u, sem],
            recv_sem=xrecv.at[u, sem],
            device_id={"tp": where},
            device_id_type=MESH,
        )

    first, second = pl.ds(0, half), pl.ds(half, half)

    def spread(u, slots):
        own, from_l, from_r = xg.at[u, t], xg.at[u, tl], xg.at[u, tr]
        opp_l, opp_r = xg.at[u, to, :, first], xg.at[u, to, :, second]
        sent = [
            x_copy(u, 1, own, own, tr),
            x_copy(u, 2, own, own, tl),
            x_copy(u, 0, own, own, partner),
        ]
        for copy in sent:
            copy.start()
        ring.pump_to(slots[0])
        more = []
        x_copy(u, 1, from_l, from_l, tr).wait_recv()
        more.append(x_copy(u, 3, from_l.at[:, first], from_l.at[:, first], tr))
        more.append(x_copy(u, 5, from_l, from_l, partner))
        more[0].start()
        x_copy(u, 2, from_r, from_r, tl).wait_recv()
        more.append(x_copy(u, 4, from_r.at[:, second], from_r.at[:, second], tl))
        more.append(x_copy(u, 6, from_r, from_r, partner))
        for copy in more[2:3] + more[1:2] + more[3:4]:
            copy.start()
        sent += more
        ring.pump_to(slots[1])
        x_copy(u, 3, opp_l, opp_l, tr).wait_recv()
        last = [x_copy(u, 7, opp_l, opp_l, partner)]
        last[0].start()
        x_copy(u, 4, opp_r, opp_r, tl).wait_recv()
        last.append(x_copy(u, 8, opp_r, opp_r, partner))
        last[1].start()
        sent += last
        ring.pump_to(slots[2])
        other = 1 - 2 * c
        for sem, ref in (
            (0, xg.at[u, partner]),
            (5, xg.at[u, tl + other]),
            (6, xg.at[u, tr + other]),
            (7, xg.at[u, to + other, :, first]),
            (8, xg.at[u, to + other, :, second]),
        ):
            x_copy(u, sem, ref, ref, partner).wait_recv()
        for chip in range(chips):
            a, b, base = xg.at[u, 2 * chip], xg.at[u, 2 * chip + 1], chip * chip_rows
            lhs[base : base + 32, :] = a[0:32, :]
            lhs[base + 32 : base + 48, :] = a[32:48, :] + b[0:16, :]
            lhs[base + 48 : base + 80, :] = b[16:48, :]
        return sent

    def chip_rows_at(v):
        return pl.ds(pl.multiple_of(v * chip_rows, 16), chip_rows)

    q0, q1 = pl.ds(0, quarter), pl.ds(quarter, quarter)

    def collect(u, slots):
        mine_h = pl.ds(pl.multiple_of(c * half, half), half)
        other_h = pl.ds(pl.multiple_of((1 - c) * half, half), half)
        sent = [x_copy(u, 9, prod.at[u, :, other_h], din.at[u], partner)]
        sent[0].start()
        ring.pump_to(slots[0])
        x_copy(u, 9, prod.at[u, :, other_h], din.at[u], partner).wait_recv()
        psum[u, :, :] = (
            prod[u, :, mine_h].astype(F32) + din[u, :, :].astype(F32)
        ).astype(BF16)
        plan = [
            (10, psum.at[u, chip_rows_at(xo), q0], opp.at[u, 0], tr),
            (11, psum.at[u, chip_rows_at(xo), q1], opp.at[u, 1], tl),
            (12, psum.at[u, chip_rows_at(xr), q1], near.at[u, 0, 1], tr),
            (13, psum.at[u, chip_rows_at(xl), q0], near.at[u, 1, 0], tl),
        ]
        for item in plan:
            copy = x_copy(u, *item)
            copy.start()
            sent.append(copy)
        ring.pump_to(slots[1])
        for way, sem, v, q, where in ((0, 10, xr, q0, tr), (1, 11, xl, q1, tl)):
            x_copy(u, sem, psum.at[u, chip_rows_at(xo), q], opp.at[u, way], where).wait_recv()
            comb[u, way, :, :] = (
                psum[u, chip_rows_at(v), q].astype(F32) + opp[u, way, :, :].astype(F32)
            ).astype(BF16)
            copy = x_copy(u, 14 + way, comb.at[u, way], near.at[u, way, way], where)
            copy.start()
            sent.append(copy)
        ring.pump_to(slots[2])
        for sem, way, part, where in ((12, 0, 1, tr), (13, 1, 0, tl), (14, 0, 0, tr), (15, 1, 1, tl)):
            x_copy(u, sem, comb.at[u, way], near.at[u, way, part], where).wait_recv()
        for part, q in ((0, q0), (1, q1)):
            fin[u, :, q] = (
                psum[u, chip_rows_at(x), q].astype(F32)
                + near[u, 0, part, :, :].astype(F32)
                + near[u, 1, part, :, :].astype(F32)
            )
        mine_r = pl.ds(pl.multiple_of(c * rows, 8), rows)
        other_r = pl.ds(pl.multiple_of((1 - c) * rows, 8), rows)
        copy = x_copy(u, 16, fin.at[u, other_r, :], got.at[u], partner)
        copy.start()
        sent.append(copy)
        ring.pump_to(slots[3])
        copy.wait_recv()
        here, there = fin[u, mine_r, :], got[u, :, :]
        return jnp.where(odd, there, here), jnp.where(odd, here, there), sent

    left = tokens[:, 0:half].astype(F32)
    right = tokens[:, half:width].astype(F32)
    put_normed(0, left, right, mix_gain)
    cgain[...] = chan_gain[...].astype(F32).reshape(1, -1)
    pl.semaphore_wait(barrier, tp + 2)
    for load in loads:
        load.wait()
    ring.pump_to(1)
    sent = spread(0, (2, 4, 5))

    ring.finish([0])
    ring.pump()
    both = jnp.dot(lhs[...], vg[...], preferred_element_type=F32)
    glu = (both[:, 0:LANES] * jax.nn.sigmoid(both[:, LANES:PAIR])).astype(BF16).astype(F32)
    segments = group_rows // LEN
    taps_n = conv_taps.shape[0]
    cbuf[:, 0:PAD_ROWS, :] = jnp.zeros((segments, PAD_ROWS, LANES), F32)
    for s in range(segments):
        cbuf[s, PAD_ROWS:, :] = glu[s * LEN : (s + 1) * LEN, :]
    my_ch = pl.ds(pl.multiple_of(t * LANES, LANES), LANES)
    taps = conv_taps[:, my_ch].astype(F32)

    def convolve(s, z):
        total = jnp.zeros((LEN, LANES), F32)
        for k in range(taps_n):
            at = PAD_ROWS - (taps_n - 1) + k
            total = total + cbuf[s, at : at + LEN, :] * taps[k : k + 1, :]
        conv[pl.ds(pl.multiple_of(s * LEN, LEN), LEN), :] = total
        return z

    lax.fori_loop(0, segments, convolve, 0)
    conv_out = conv[...]
    ring.pump()
    ones = jnp.ones((8, LANES), F32)
    high = lax.Precision.HIGHEST
    sums = lax.dot_general(ones, conv_out, NT, precision=high, preferred_element_type=F32)
    squares = lax.dot_general(
        ones, conv_out * conv_out, NT, precision=high, preferred_element_type=F32
    )
    pick = lax.broadcasted_iota(jnp.int32, (8, group_rows), 0) < 4
    stats[t, :, 0:group_rows] = jnp.where(pick, sums, squares)

    def stat_copy(d):
        return pltpu.make_async_remote_copy(
            src_ref=stats.at[t],
            dst_ref=stats.at[t],
            send_sem=ssend.at[d - 1],
            recv_sem=srecv.at[d - 1],
            device_id={"tp": lax.rem(t + d, tp)},
            device_id_type=MESH,
        )

    stat_copies = [stat_copy(d) for d in range(1, tp)]
    for copy in stat_copies:
        copy.start()
    ring.pump()
    for d in range(1, tp):
        source = lax.rem(t + tp - d, tp)
        pltpu.make_async_remote_copy(
            src_ref=stats.at[source],
            dst_ref=stats.at[source],
            send_sem=ssend.at[d - 1],
            recv_sem=srecv.at[d - 1],
            device_id={"tp": source},
            device_id_type=MESH,
        ).wait_recv()
    channels = chan_gain.shape[0]
    both_stats = jnp.sum(stats[:, :, 0:group_rows], axis=0) / channels
    flipped = jnp.transpose(
        jnp.concatenate([both_stats] + [jnp.zeros((8, group_rows), F32)] * 15, axis=0)
    )
    mean, square = flipped[:, 0:1], flipped[:, 4:5]
    scale = lax.rsqrt(square - mean * mean + chan_epsilon)
    normal = (conv_out - mean) * scale * cgain[:, my_ch]
    activated = (normal * jax.nn.sigmoid(normal)).astype(BF16)
    wide = min(512, width)
    for j in range(width // wide):
        prod[0, :, j * wide : (j + 1) * wide] = lax.dot_general(
            activated, outt[j * wide : (j + 1) * wide, :], NT, preferred_element_type=F32
        ).astype(BF16)

    ring.pump()
    base = ring.at
    left_sum, right_sum, more = collect(0, (base + 1, base + 3, base + 5, base + 6))
    sent += more

    def rms(a, b, gain):
        scale = lax.rsqrt(
            (jnp.sum(a * a, axis=1, keepdims=True) + jnp.sum(b * b, axis=1, keepdims=True)) / width
            + norm_epsilon
        )
        return (
            a * scale * gain[0:half].astype(F32).reshape(1, half),
            b * scale * gain[half:width].astype(F32).reshape(1, half),
        )

    a, b = rms(left_sum, right_sum, mix_post_gain)
    res_a = (tokens[:, 0:half].astype(F32) + a).astype(BF16)
    res_b = (tokens[:, half:width].astype(F32) + b).astype(BF16)
    resid[:, 0:half] = res_a.astype(F32)
    resid[:, half:width] = res_b.astype(F32)
    put_normed(1, res_a.astype(F32), res_b.astype(F32), ffn_gain)
    base = ring.at
    sent += spread(1, (base + 1, base + 2, base + 3))
    ring.pump_to(ring.last)

    fbuf[:, 0:FPAD, :] = jnp.zeros((segments, FPAD, PAIR), F32)
    ftaps_n = ffn_taps.shape[0]

    def feed(j):
        pair = jnp.dot(lhs[...], up[j], preferred_element_type=F32).astype(BF16).astype(F32)
        for s in range(segments):
            fbuf[s, FPAD:, :] = pair[s * LEN : (s + 1) * LEN, :]
        here = pl.ds(pl.multiple_of(t * (pieces * LANES) + j * LANES, LANES), LANES)
        gate_taps = ffn_taps[:, 0, here].astype(F32)
        val_taps = ffn_taps[:, 1, here].astype(F32)
        for s in range(segments):
            gate = jnp.zeros((LEN, LANES), F32)
            val = jnp.zeros((LEN, LANES), F32)
            for k in range(ftaps_n):
                at = FPAD - (ftaps_n - 1) + k
                gate = gate + fbuf[s, at : at + LEN, 0:LANES] * gate_taps[k : k + 1, :]
                val = val + fbuf[s, at : at + LEN, LANES:PAIR] * val_taps[k : k + 1, :]
            hidden[j, s * LEN : (s + 1) * LEN, :] = (
                jax.nn.gelu(gate, approximate=True) * val
            ).astype(BF16)

    for j in own + both_sides:
        feed(j)
    for at, j in zip(own_at, far):
        ring.handed(at, up.at[j, 0 : (n - 1) * block, :])
        feed(j)
    ring.handed(down_at, downt.at[0 : (n - 1) * (block // 2), :])

    def contract(j, z):
        columns = pl.ds(pl.multiple_of(j * PAIR, PAIR), PAIR)
        units = jnp.concatenate([hidden[i] for i in range(pieces)], axis=1)
        prod[1, :, columns] = lax.dot_general(
            units, downt[columns, :], NT, preferred_element_type=F32
        ).astype(BF16)
        return z

    lax.fori_loop(0, width // PAIR, contract, 0)
    left_sum, right_sum, more = collect(1, (0, 0, 0, 0))
    sent += more
    a, b = rms(left_sum, right_sum, ffn_post_gain)
    out[:, 0:half] = (resid[:, 0:half] + a).astype(BF16)
    out[:, half:width] = (resid[:, half:width] + b).astype(BF16)

    for copy in sent + stat_copies:
        copy.wait_send()

    def whole_of(buffer, size, count):
        return buffer.at[pl.ds(0, count * size), :]

    wholes = [functools.partial(whole_of, vg, block), functools.partial(whole_of, outt, block)]
    wholes += [functools.partial(whole_of, up.at[0], block)] * share
    wholes += [functools.partial(whole_of, downt, block // 2)]
    wholes += [functools.partial(whole_of, up.at[0], block)] * len(both_sides)
    ring.drain(wholes)


def shards(*args):
    tokens, up_weight = args[0], args[9]
    n, tp = lax.axis_size("fs"), lax.axis_size("tp")
    rows, width = tokens.shape
    half, quarter = width // 2, width // 4
    group_rows, chip_rows = rows * tp, 2 * rows
    segments = group_rows // LEN
    pieces = up_weight.shape[1] // LANES
    streams = 3 + pieces - pieces // 2
    steps = n // 2
    args = list(args)
    args[6], args[12], args[11] = args[6].T, args[12].T, args[11].transpose(1, 0, 2)
    vmem = pl.BlockSpec(memory_space=pltpu.VMEM)
    hbm = pl.BlockSpec(memory_space=pltpu.HBM)
    dma = pltpu.SemaphoreType.DMA
    return pl.pallas_call(
        functools.partial(layer_kernel, n, tp),
        out_shape=jax.ShapeDtypeStruct((rows, width), BF16),
        in_specs=[hbm if i in (2, 3, 6, 9, 10, 12) else vmem for i in range(len(args))],
        out_specs=vmem,
        scratch_shapes=[
            pltpu.VMEM((width, PAIR), BF16),
            pltpu.VMEM((width, LANES), BF16),
            pltpu.VMEM((pieces, width, PAIR), BF16),
            pltpu.VMEM((width, pieces * LANES), BF16),
            pltpu.VMEM((2, tp, rows + 8, width), BF16),
            pltpu.VMEM((group_rows, width), BF16),
            pltpu.VMEM((2, group_rows, width), BF16),
            pltpu.VMEM((2, group_rows, half), BF16),
            pltpu.VMEM((2, group_rows, half), BF16),
            pltpu.VMEM((2, 2, chip_rows, quarter), BF16),
            pltpu.VMEM((2, 2, 2, chip_rows, quarter), BF16),
            pltpu.VMEM((2, 2, chip_rows, quarter), BF16),
            pltpu.VMEM((2, chip_rows, half), F32),
            pltpu.VMEM((2, rows, half), F32),
            pltpu.VMEM((segments, PAD_ROWS + LEN, LANES), F32),
            pltpu.VMEM((group_rows, LANES), F32),
            pltpu.VMEM((tp, 8, pl.cdiv(group_rows, LANES) * LANES), F32),
            pltpu.VMEM((rows, width), F32),
            pltpu.VMEM((segments, FPAD + LEN, PAIR), F32),
            pltpu.VMEM((pieces, group_rows, LANES), BF16),
            pltpu.VMEM((1, args[5].shape[0]), F32),
            dma((4 + 2 * pieces,)),
            dma((streams, 2)),
            dma((streams, 2, steps)),
            dma((streams,)),
            dma((streams,)),
            dma((2, 17)),
            dma((2, 17)),
            dma((tp - 1,)),
            dma((tp - 1,)),
        ],
        compiler_params=pltpu.CompilerParams(
            collective_id=0, has_side_effects=True, vmem_limit_bytes=60 * 1024 * 1024
        ),
    )(*args)


def solution(mesh):
    return jax.shard_map(
        shards,
        mesh=mesh,
        in_specs=(
            P(("grp", "fs", "tp"), None),
            P(),
            P("fs", "tp"),
            P("fs", "tp"),
            P(),
            P(),
            P("tp", "fs"),
            P(),
            P(),
            P("fs", "tp"),
            P("fs", "tp"),
            P(),
            P("tp", "fs"),
            P(),
        ),
        out_specs=P(("grp", "fs", "tp"), None),
        check_vma=False,
    )
```

```python
import functools

import jax
import jax.numpy as jnp
from jax import lax
from jax.experimental import pallas as pl
from jax.experimental.pallas import tpu as pltpu
from jax.sharding import PartitionSpec as P

LEN = 64
MESH = pl.DeviceIdType.MESH
F32 = jnp.float32
BF16 = jnp.bfloat16
NT = (((1,), (1,)), ((), ()))

norm_epsilon = 1e-06
chan_epsilon = 1e-05

LANES = 128
PAIR = 2 * LANES
PAD_ROWS = 32
LATE = 0
FPAD = 8


class Ring:
    def __init__(self, n, me, streams, offsets, strides, shared, mate, sems):
        self.n, self.me = n, me
        self.streams, self.offsets, self.strides = streams, offsets, strides
        self.shared, self.mate = shared, mate
        self.send_sem, self.recv_sem, self.ysend, self.yrecv = sems
        self.reach = (n // 2, (n - 1) - n // 2)
        self.at = 0
        self.last = max(self.end(j) for j in range(len(streams)))

    def end(self, j):
        return self.offsets[j] + pl.cdiv(self.reach[0], self.strides[j]) + 1

    def place(self, way, distance):
        shift = distance if way == 0 else self.n - distance
        return lax.rem(self.me + shift, self.n)

    def copy(self, j, way, owner, hop, distance):
        ref = self.streams[j](owner)
        return pltpu.make_async_remote_copy(
            src_ref=ref,
            dst_ref=ref,
            send_sem=self.send_sem.at[j, way],
            recv_sem=self.recv_sem.at[j, way, distance - 1],
            device_id={"fs": self.place(way, hop)},
            device_id_type=MESH,
        )

    def across(self, j, owner):
        if j in self.shared:
            ref = self.streams[j](owner)
            pltpu.make_async_remote_copy(
                src_ref=ref,
                dst_ref=ref,
                send_sem=self.ysend.at[j],
                recv_sem=self.yrecv.at[j],
                device_id={"grp": self.mate},
                device_id_type=MESH,
            ).start()

    def step(self, j, way, distance, forward):
        hop = self.strides[j]
        owner = self.place(1 - way, distance)
        self.copy(j, way, owner, hop, distance).wait_recv()
        if forward:
            self.copy(j, way, owner, hop, distance + hop).start()
        self.across(j, owner)

    def slot(self, k):
        for j, off in enumerate(self.offsets):
            hop, turn = self.strides[j], k - off
            for way in (0, 1):
                if turn == 0:
                    for far in range(1, min(hop, self.reach[way]) + 1):
                        self.copy(j, way, self.me, far, far).start()
            for i in range(1, hop + 1):
                for way in (0, 1):
                    distance = (turn - 1) * hop + i
                    if turn > 0 and distance <= self.reach[way]:
                        self.step(j, way, distance, distance + hop <= self.reach[way])

    def slot_loop(self, k, active):
        for j in active:
            hop = self.strides[j]
            for i in range(1, hop + 1):
                for way in (0, 1):
                    self.step(j, way, (k - self.offsets[j] - 1) * hop + i, True)

    def kinds(self, k):
        passing, other = [], False
        for j, off in enumerate(self.offsets):
            turn = k - off
            if turn > 0 and (turn + 1) * self.strides[j] <= self.reach[1]:
                passing.append(j)
            elif 0 <= turn and k < self.end(j):
                other = True
        return tuple(passing), other

    def pump_to(self, upto):
        upto = min(upto, self.last)
        while self.at < upto:
            kinds = self.kinds(self.at)
            end = self.at + 1
            while end < upto and not kinds[1] and self.kinds(end) == kinds:
                end += 1
            if end - self.at > 1:
                lax.fori_loop(
                    self.at, end, lambda k, z, on=kinds[0]: (self.slot_loop(k, on), z)[1], 0
                )
            else:
                self.slot(self.at)
            self.at = end

    def pump(self, count=1):
        self.pump_to(self.at + count)

    def finish(self, js):
        self.pump_to(max(self.end(j) for j in js))

    def handed(self, j, whole):
        pltpu.make_async_copy(whole, whole, self.yrecv.at[j]).wait()

    def drain(self, wholes):
        for j, whole in enumerate(wholes):
            for way in (0, 1):
                if self.reach[way] > 0:
                    ref = whole(self.reach[way])
                    pltpu.make_async_copy(ref, ref, self.send_sem.at[j, way]).wait()
            if j in self.shared:
                ref = whole(self.n - 1)
                pltpu.make_async_copy(ref, ref, self.ysend.at[j]).wait()


def layer_kernel(
    n,
    tp,
    tokens,
    mix_gain,
    val_h,
    gate_h,
    conv_taps,
    chan_gain,
    out_h,
    mix_post_gain,
    ffn_gain,
    up_gate_h,
    up_val_h,
    ffn_taps,
    down_h,
    ffn_post_gain,
    out,
    vg,
    outt,
    up,
    downt,
    xg,
    lhs,
    prod,
    din,
    psum,
    opp,
    near,
    comb,
    fin,
    got,
    cbuf,
    conv,
    stats,
    resid,
    fbuf,
    hidden,
    cgain,
    load_sem,
    zsend,
    zrecv,
    ysend,
    yrecv,
    xsend,
    xrecv,
    ssend,
    srecv,
):
    rows, width = tokens.shape
    half, quarter = width // 2, width // 4
    block = width // n
    group_rows = rows * tp
    chip_rows = 2 * rows
    chips = tp // 2
    pieces = up_gate_h.shape[1] // LANES
    f = lax.axis_index("fs")
    t = lax.axis_index("tp")
    x, c = t // 2, lax.rem(t, 2)
    partner = t + 1 - 2 * c
    xr, xl, xo = (lax.rem(x + s, chips) for s in (1, chips - 1, 2))
    tr, tl, to = (2 * v + c for v in (xr, xl, xo))
    odd = c == 1
    g = lax.axis_index("grp")
    side = lax.rem(g, 2)
    mate = g + 1 - 2 * side

    mine = pl.ds(pl.multiple_of(f * block, block), block)
    loads = [
        pltpu.make_async_copy(val_h, vg.at[mine, pl.ds(0, LANES)], load_sem.at[0]),
        pltpu.make_async_copy(gate_h, vg.at[mine, pl.ds(LANES, LANES)], load_sem.at[1]),
    ]
    for j in range(pieces):
        columns = pl.ds(j * LANES, LANES)
        loads.append(
            pltpu.make_async_copy(
                up_gate_h.at[:, columns], up.at[j, mine, pl.ds(0, LANES)], load_sem.at[2 + 2 * j]
            )
        )
        loads.append(
            pltpu.make_async_copy(
                up_val_h.at[:, columns], up.at[j, mine, pl.ds(LANES, LANES)], load_sem.at[3 + 2 * j]
            )
        )
    loads.append(pltpu.make_async_copy(out_h, outt.at[mine, :], load_sem.at[2 + 2 * pieces]))
    loads.append(pltpu.make_async_copy(down_h, downt.at[mine, :], load_sem.at[3 + 2 * pieces]))
    for load in loads:
        load.start()

    barrier = pltpu.get_barrier_semaphore()
    for z in (1, 2, n - 2, n - 1):
        pl.semaphore_signal(barrier, inc=1, device_id={"fs": lax.rem(f + z, n)}, device_id_type=MESH)
    for d in range(1, tp):
        pl.semaphore_signal(
            barrier, inc=1, device_id={"tp": lax.rem(t + d, tp)}, device_id_type=MESH
        )

    pl.semaphore_signal(barrier, inc=1, device_id={"grp": mate}, device_id_type=MESH)

    def zview(buffer, owner):
        return buffer.at[pl.ds(pl.multiple_of(owner * block, block), block), :]

    def down_view(part, owner):
        size = block // 2
        start = pl.multiple_of(owner * block + part * size, size)
        return downt.at[pl.ds(start, size), :]

    share = pieces // 2
    own = [side * share + i for i in range(share)]
    far = [(1 - side) * share + i for i in range(share)]
    both_sides = list(range(2 * share, pieces))
    streams = [functools.partial(zview, vg), functools.partial(zview, outt)]
    streams += [functools.partial(zview, up.at[j]) for j in own]
    streams += [functools.partial(down_view, side)]
    streams += [functools.partial(zview, up.at[j]) for j in both_sides]
    own_at = list(range(2, 2 + share))
    down_at = 2 + share
    both_at = list(range(down_at + 1, len(streams)))
    offsets = [0, min(3, n // 2)] + [0] * share + [min(LATE, n // 2)] * (1 + len(both_sides))
    strides = [2, 2] + [1] * (len(streams) - 2)
    ring = Ring(n, f, streams, offsets, strides, own_at + [down_at], mate, (zsend, zrecv, ysend, yrecv))

    def put_normed(u, left, right, gain):
        scale = lax.rsqrt(
            (
                jnp.sum(left * left, axis=1, keepdims=True)
                + jnp.sum(right * right, axis=1, keepdims=True)
            )
            / width
            + norm_epsilon
        )
        pad = jnp.zeros((8, half), F32)
        for at, part in ((0, left), (half, right)):
            value = part * scale * gain[at : at + half].astype(F32).reshape(1, half)
            low = jnp.concatenate([value, pad], axis=0)
            high = jnp.concatenate([pad, value], axis=0)
            xg[u, t, :, at : at + half] = jnp.where(odd, high, low).astype(BF16)

    def x_copy(u, sem, src, dst, where):
        return pltpu.make_async_remote_copy(
            src_ref=src,
            dst_ref=dst,
            send_sem=xsend.at[u, sem],
            recv_sem=xrecv.at[u, sem],
            device_id={"tp": where},
            device_id_type=MESH,
        )

    first, second = pl.ds(0, half), pl.ds(half, half)

    def spread(u, slots):
        own, from_l, from_r = xg.at[u, t], xg.at[u, tl], xg.at[u, tr]
        opp_l, opp_r = xg.at[u, to, :, first], xg.at[u, to, :, second]
        sent = [
            x_copy(u, 1, own, own, tr),
            x_copy(u, 2, own, own, tl),
            x_copy(u, 0, own, own, partner),
        ]
        for copy in sent:
            copy.start()
        ring.pump_to(slots[0])
        more = []
        x_copy(u, 1, from_l, from_l, tr).wait_recv()
        more.append(x_copy(u, 3, from_l.at[:, first], from_l.at[:, first], tr))
        more.append(x_copy(u, 5, from_l, from_l, partner))
        more[0].start()
        x_copy(u, 2, from_r, from_r, tl).wait_recv()
        more.append(x_copy(u, 4, from_r.at[:, second], from_r.at[:, second], tl))
        more.append(x_copy(u, 6, from_r, from_r, partner))
        for copy in more[2:3] + more[1:2] + more[3:4]:
            copy.start()
        sent += more
        ring.pump_to(slots[1])
        x_copy(u, 3, opp_l, opp_l, tr).wait_recv()
        last = [x_copy(u, 7, opp_l, opp_l, partner)]
        last[0].start()
        x_copy(u, 4, opp_r, opp_r, tl).wait_recv()
        last.append(x_copy(u, 8, opp_r, opp_r, partner))
        last[1].start()
        sent += last
        ring.pump_to(slots[2])
        other = 1 - 2 * c
        for sem, ref in (
            (0, xg.at[u, partner]),
            (5, xg.at[u, tl + other]),
            (6, xg.at[u, tr + other]),
            (7, xg.at[u, to + other, :, first]),
            (8, xg.at[u, to + other, :, second]),
        ):
            x_copy(u, sem, ref, ref, partner).wait_recv()
        for chip in range(chips):
            a, b, base = xg.at[u, 2 * chip], xg.at[u, 2 * chip + 1], chip * chip_rows
            lhs[base : base + 32, :] = a[0:32, :]
            lhs[base + 32 : base + 48, :] = a[32:48, :] + b[0:16, :]
            lhs[base + 48 : base + 80, :] = b[16:48, :]
        return sent

    def chip_rows_at(v):
        return pl.ds(pl.multiple_of(v * chip_rows, 16), chip_rows)

    q0, q1 = pl.ds(0, quarter), pl.ds(quarter, quarter)

    mine_h = pl.ds(pl.multiple_of(c * half, half), half)
    other_h = pl.ds(pl.multiple_of((1 - c) * half, half), half)

    def multiply(u, left, weight, wide):
        sent = x_copy(u, 9, prod.at[u, :, other_h], din.at[u], partner)
        for side_at in (1 - c, c):

            def piece(j, z, side_at=side_at):
                columns = pl.ds(pl.multiple_of(side_at * half + j * wide, wide), wide)
                prod[u, :, columns] = lax.dot_general(
                    left, weight[columns, :], NT, preferred_element_type=F32
                ).astype(BF16)
                return z

            lax.fori_loop(0, half // wide, piece, 0)
            if side_at is not c:
                sent.start()
        return sent

    def collect(u, handed, slots):
        sent = [handed]
        ring.pump_to(slots[0])
        x_copy(u, 9, prod.at[u, :, other_h], din.at[u], partner).wait_recv()
        psum[u, :, :] = (
            prod[u, :, mine_h].astype(F32) + din[u, :, :].astype(F32)
        ).astype(BF16)
        plan = [
            (10, psum.at[u, chip_rows_at(xo), q0], opp.at[u, 0], tr),
            (11, psum.at[u, chip_rows_at(xo), q1], opp.at[u, 1], tl),
            (12, psum.at[u, chip_rows_at(xr), q1], near.at[u, 0, 1], tr),
            (13, psum.at[u, chip_rows_at(xl), q0], near.at[u, 1, 0], tl),
        ]
        for item in plan:
            copy = x_copy(u, *item)
            copy.start()
            sent.append(copy)
        ring.pump_to(slots[1])
        for way, sem, v, q, where in ((0, 10, xr, q0, tr), (1, 11, xl, q1, tl)):
            x_copy(u, sem, psum.at[u, chip_rows_at(xo), q], opp.at[u, way], where).wait_recv()
            comb[u, way, :, :] = (
                psum[u, chip_rows_at(v), q].astype(F32) + opp[u, way, :, :].astype(F32)
            ).astype(BF16)
            copy = x_copy(u, 14 + way, comb.at[u, way], near.at[u, way, way], where)
            copy.start()
            sent.append(copy)
        ring.pump_to(slots[2])
        for sem, way, part, where in ((12, 0, 1, tr), (13, 1, 0, tl), (14, 0, 0, tr), (15, 1, 1, tl)):
            x_copy(u, sem, comb.at[u, way], near.at[u, way, part], where).wait_recv()
        for part, q in ((0, q0), (1, q1)):
            fin[u, :, q] = (
                psum[u, chip_rows_at(x), q].astype(F32)
                + near[u, 0, part, :, :].astype(F32)
                + near[u, 1, part, :, :].astype(F32)
            )
        mine_r = pl.ds(pl.multiple_of(c * rows, 8), rows)
        other_r = pl.ds(pl.multiple_of((1 - c) * rows, 8), rows)
        copy = x_copy(u, 16, fin.at[u, other_r, :], got.at[u], partner)
        copy.start()
        sent.append(copy)
        ring.pump_to(slots[3])
        copy.wait_recv()
        here, there = fin[u, mine_r, :], got[u, :, :]
        return jnp.where(odd, there, here), jnp.where(odd, here, there), sent

    left = tokens[:, 0:half].astype(F32)
    right = tokens[:, half:width].astype(F32)
    put_normed(0, left, right, mix_gain)
    cgain[...] = chan_gain[...].astype(F32).reshape(1, -1)
    pl.semaphore_wait(barrier, tp + 4)
    for load in loads:
        load.wait()
    ring.pump_to(1)
    sent = spread(0, (3, 4, 5))

    ring.finish([0])
    ring.pump()
    both = jnp.dot(lhs[...], vg[...], preferred_element_type=F32)
    glu = (both[:, 0:LANES] * jax.nn.sigmoid(both[:, LANES:PAIR])).astype(BF16).astype(F32)
    segments = group_rows // LEN
    taps_n = conv_taps.shape[0]
    cbuf[:, 0:PAD_ROWS, :] = jnp.zeros((segments, PAD_ROWS, LANES), F32)
    for s in range(segments):
        cbuf[s, PAD_ROWS:, :] = glu[s * LEN : (s + 1) * LEN, :]
    my_ch = pl.ds(pl.multiple_of(t * LANES, LANES), LANES)
    taps = conv_taps[:, my_ch].astype(F32)

    def convolve(s, z):
        total = jnp.zeros((LEN, LANES), F32)
        for k in range(taps_n):
            at = PAD_ROWS - (taps_n - 1) + k
            total = total + cbuf[s, at : at + LEN, :] * taps[k : k + 1, :]
        conv[pl.ds(pl.multiple_of(s * LEN, LEN), LEN), :] = total
        return z

    lax.fori_loop(0, segments, convolve, 0)
    conv_out = conv[...]
    ring.pump(1)
    ones = jnp.ones((8, LANES), F32)
    high = lax.Precision.HIGHEST
    sums = lax.dot_general(ones, conv_out, NT, precision=high, preferred_element_type=F32)
    squares = lax.dot_general(
        ones, conv_out * conv_out, NT, precision=high, preferred_element_type=F32
    )
    pick = lax.broadcasted_iota(jnp.int32, (8, group_rows), 0) < 4
    stats[t, :, 0:group_rows] = jnp.where(pick, sums, squares)

    def stat_copy(d):
        return pltpu.make_async_remote_copy(
            src_ref=stats.at[t],
            dst_ref=stats.at[t],
            send_sem=ssend.at[d - 1],
            recv_sem=srecv.at[d - 1],
            device_id={"tp": lax.rem(t + d, tp)},
            device_id_type=MESH,
        )

    stat_copies = [stat_copy(d) for d in range(1, tp)]
    for copy in stat_copies:
        copy.start()
    ring.pump(0)
    for d in range(1, tp):
        source = lax.rem(t + tp - d, tp)
        pltpu.make_async_remote_copy(
            src_ref=stats.at[source],
            dst_ref=stats.at[source],
            send_sem=ssend.at[d - 1],
            recv_sem=srecv.at[d - 1],
            device_id={"tp": source},
            device_id_type=MESH,
        ).wait_recv()
    channels = chan_gain.shape[0]
    both_stats = jnp.sum(stats[:, :, 0:group_rows], axis=0) / channels
    flipped = jnp.transpose(
        jnp.concatenate([both_stats] + [jnp.zeros((8, group_rows), F32)] * 15, axis=0)
    )
    mean, square = flipped[:, 0:1], flipped[:, 4:5]
    scale = lax.rsqrt(square - mean * mean + chan_epsilon)
    normal = (conv_out - mean) * scale * cgain[:, my_ch]
    activated = (normal * jax.nn.sigmoid(normal)).astype(BF16)
    ring.finish([1])
    handed = multiply(0, activated, outt, min(512, half))
    ring.pump(1)
    base = ring.at
    left_sum, right_sum, more = collect(0, handed, (base + 0, base + 1, base + 1, base + 2))
    sent += more

    def rms(a, b, gain):
        scale = lax.rsqrt(
            (jnp.sum(a * a, axis=1, keepdims=True) + jnp.sum(b * b, axis=1, keepdims=True)) / width
            + norm_epsilon
        )
        return (
            a * scale * gain[0:half].astype(F32).reshape(1, half),
            b * scale * gain[half:width].astype(F32).reshape(1, half),
        )

    a, b = rms(left_sum, right_sum, mix_post_gain)
    res_a = (tokens[:, 0:half].astype(F32) + a).astype(BF16)
    res_b = (tokens[:, half:width].astype(F32) + b).astype(BF16)
    resid[:, 0:half] = res_a.astype(F32)
    resid[:, half:width] = res_b.astype(F32)
    put_normed(1, res_a.astype(F32), res_b.astype(F32), ffn_gain)
    base = ring.at
    sent += spread(1, (base + 1, base + 2, base + 2))

    fbuf[:, 0:FPAD, :] = jnp.zeros((segments, FPAD, PAIR), F32)
    ftaps_n = ffn_taps.shape[0]

    def feed(j):
        pair = jnp.dot(lhs[...], up[j], preferred_element_type=F32).astype(BF16).astype(F32)
        for s in range(segments):
            fbuf[s, FPAD:, :] = pair[s * LEN : (s + 1) * LEN, :]
        here = pl.ds(pl.multiple_of(t * (pieces * LANES) + j * LANES, LANES), LANES)
        gate_taps = ffn_taps[:, 0, here].astype(F32)
        val_taps = ffn_taps[:, 1, here].astype(F32)
        for s in range(segments):
            gate = jnp.zeros((LEN, LANES), F32)
            val = jnp.zeros((LEN, LANES), F32)
            for k in range(ftaps_n):
                at = FPAD - (ftaps_n - 1) + k
                gate = gate + fbuf[s, at : at + LEN, 0:LANES] * gate_taps[k : k + 1, :]
                val = val + fbuf[s, at : at + LEN, LANES:PAIR] * val_taps[k : k + 1, :]
            hidden[j, s * LEN : (s + 1) * LEN, :] = (
                jax.nn.gelu(gate, approximate=True) * val
            ).astype(BF16)

    ring.finish(own_at)
    for j in own:
        feed(j)
        ring.pump()
    ring.pump_to(ring.last)
    for j in both_sides:
        feed(j)
    for at, j in zip(own_at, far):
        ring.handed(at, up.at[j, 0 : (n - 1) * block, :])
        feed(j)
    ring.handed(down_at, downt.at[0 : (n - 1) * (block // 2), :])

    units = jnp.concatenate([hidden[i] for i in range(pieces)], axis=1)
    handed = multiply(1, units, downt, min(PAIR, half))
    left_sum, right_sum, more = collect(1, handed, (0, 0, 0, 0))
    sent += more
    a, b = rms(left_sum, right_sum, ffn_post_gain)
    out[:, 0:half] = (resid[:, 0:half] + a).astype(BF16)
    out[:, half:width] = (resid[:, half:width] + b).astype(BF16)

    for copy in sent + stat_copies:
        copy.wait_send()

    def whole_of(buffer, size, count):
        return buffer.at[pl.ds(0, count * size), :]

    wholes = [functools.partial(whole_of, vg, block), functools.partial(whole_of, outt, block)]
    wholes += [functools.partial(whole_of, up.at[0], block)] * share
    wholes += [functools.partial(whole_of, downt, block // 2)]
    wholes += [functools.partial(whole_of, up.at[0], block)] * len(both_sides)
    ring.drain(wholes)


def shards(*args):
    tokens, up_weight = args[0], args[9]
    n, tp = lax.axis_size("fs"), lax.axis_size("tp")
    rows, width = tokens.shape
    half, quarter = width // 2, width // 4
    group_rows, chip_rows = rows * tp, 2 * rows
    segments = group_rows // LEN
    pieces = up_weight.shape[1] // LANES
    streams = 3 + pieces - pieces // 2
    steps = n // 2
    args = list(args)
    args[6], args[12], args[11] = args[6].T, args[12].T, args[11].transpose(1, 0, 2)
    vmem = pl.BlockSpec(memory_space=pltpu.VMEM)
    hbm = pl.BlockSpec(memory_space=pltpu.HBM)
    dma = pltpu.SemaphoreType.DMA
    return pl.pallas_call(
        functools.partial(layer_kernel, n, tp),
        out_shape=jax.ShapeDtypeStruct((rows, width), BF16),
        in_specs=[hbm if i in (2, 3, 6, 9, 10, 12) else vmem for i in range(len(args))],
        out_specs=vmem,
        scratch_shapes=[
            pltpu.VMEM((width, PAIR), BF16),
            pltpu.VMEM((width, LANES), BF16),
            pltpu.VMEM((pieces, width, PAIR), BF16),
            pltpu.VMEM((width, pieces * LANES), BF16),
            pltpu.VMEM((2, tp, rows + 8, width), BF16),
            pltpu.VMEM((group_rows, width), BF16),
            pltpu.VMEM((2, group_rows, width), BF16),
            pltpu.VMEM((2, group_rows, half), BF16),
            pltpu.VMEM((2, group_rows, half), BF16),
            pltpu.VMEM((2, 2, chip_rows, quarter), BF16),
            pltpu.VMEM((2, 2, 2, chip_rows, quarter), BF16),
            pltpu.VMEM((2, 2, chip_rows, quarter), BF16),
            pltpu.VMEM((2, chip_rows, half), F32),
            pltpu.VMEM((2, rows, half), F32),
            pltpu.VMEM((segments, PAD_ROWS + LEN, LANES), F32),
            pltpu.VMEM((group_rows, LANES), F32),
            pltpu.VMEM((tp, 8, pl.cdiv(group_rows, LANES) * LANES), F32),
            pltpu.VMEM((rows, width), F32),
            pltpu.VMEM((segments, FPAD + LEN, PAIR), F32),
            pltpu.VMEM((pieces, group_rows, LANES), BF16),
            pltpu.VMEM((1, args[5].shape[0]), F32),
            dma((4 + 2 * pieces,)),
            dma((streams, 2)),
            dma((streams, 2, steps)),
            dma((streams,)),
            dma((streams,)),
            dma((2, 17)),
            dma((2, 17)),
            dma((tp - 1,)),
            dma((tp - 1,)),
        ],
        compiler_params=pltpu.CompilerParams(
            collective_id=0, has_side_effects=True, vmem_limit_bytes=60 * 1024 * 1024
        ),
    )(*args)


def solution(mesh):
    return jax.shard_map(
        shards,
        mesh=mesh,
        in_specs=(
            P(("grp", "fs", "tp"), None),
            P(),
            P("fs", "tp"),
            P("fs", "tp"),
            P(),
            P(),
            P("tp", "fs"),
            P(),
            P(),
            P("fs", "tp"),
            P("fs", "tp"),
            P(),
            P("tp", "fs"),
            P(),
        ),
        out_specs=P(("grp", "fs", "tp"), None),
        check_vma=False,
    )
```

```python
import functools

import jax
import jax.numpy as jnp
from jax import lax
from jax.experimental import pallas as pl
from jax.experimental.pallas import tpu as pltpu
from jax.sharding import PartitionSpec as P

LEN = 64
MESH = pl.DeviceIdType.MESH
F32 = jnp.float32
BF16 = jnp.bfloat16
NT = (((1,), (1,)), ((), ()))

norm_epsilon = 1e-06
chan_epsilon = 1e-05

LANES = 128
PAIR = 2 * LANES
PAD_ROWS = 32
LATE = 0
FPAD = 8


class Ring:
    def __init__(self, n, me, streams, offsets, strides, shared, mate, sems):
        self.n, self.me = n, me
        self.streams, self.offsets, self.strides = streams, offsets, strides
        self.shared, self.mate = shared, mate
        self.send_sem, self.recv_sem, self.ysend, self.yrecv = sems
        self.reach = (n // 2, (n - 1) - n // 2)
        self.at = 0
        self.last = max(self.end(j) for j in range(len(streams)))

    def end(self, j):
        return self.offsets[j] + pl.cdiv(self.reach[0], self.strides[j]) + 1

    def place(self, way, distance):
        shift = distance if way == 0 else self.n - distance
        return lax.rem(self.me + shift, self.n)

    def copy(self, j, way, owner, hop, distance):
        ref = self.streams[j](owner)
        return pltpu.make_async_remote_copy(
            src_ref=ref,
            dst_ref=ref,
            send_sem=self.send_sem.at[j, way],
            recv_sem=self.recv_sem.at[j, way, distance - 1],
            device_id={"fs": self.place(way, hop)},
            device_id_type=MESH,
        )

    def across(self, j, owner):
        if j in self.shared:
            ref = self.streams[j](owner)
            pltpu.make_async_remote_copy(
                src_ref=ref,
                dst_ref=ref,
                send_sem=self.ysend.at[j],
                recv_sem=self.yrecv.at[j],
                device_id={"grp": self.mate},
                device_id_type=MESH,
            ).start()

    def step(self, j, way, distance, forward):
        hop = self.strides[j]
        owner = self.place(1 - way, distance)
        self.copy(j, way, owner, hop, distance).wait_recv()
        if forward:
            self.copy(j, way, owner, hop, distance + hop).start()
        self.across(j, owner)

    def slot(self, k):
        for j, off in enumerate(self.offsets):
            hop, turn = self.strides[j], k - off
            for way in (0, 1):
                if turn == 0:
                    for far in range(1, min(hop, self.reach[way]) + 1):
                        self.copy(j, way, self.me, far, far).start()
            for i in range(1, hop + 1):
                for way in (0, 1):
                    distance = (turn - 1) * hop + i
                    if turn > 0 and distance <= self.reach[way]:
                        self.step(j, way, distance, distance + hop <= self.reach[way])

    def slot_loop(self, k, active):
        for j in active:
            hop = self.strides[j]
            for i in range(1, hop + 1):
                for way in (0, 1):
                    self.step(j, way, (k - self.offsets[j] - 1) * hop + i, True)

    def kinds(self, k):
        passing, other = [], False
        for j, off in enumerate(self.offsets):
            turn = k - off
            if turn > 0 and (turn + 1) * self.strides[j] <= self.reach[1]:
                passing.append(j)
            elif 0 <= turn and k < self.end(j):
                other = True
        return tuple(passing), other

    def pump_to(self, upto):
        upto = min(upto, self.last)
        while self.at < upto:
            kinds = self.kinds(self.at)
            end = self.at + 1
            while end < upto and not kinds[1] and self.kinds(end) == kinds:
                end += 1
            if end - self.at > 1:
                lax.fori_loop(
                    self.at, end, lambda k, z, on=kinds[0]: (self.slot_loop(k, on), z)[1], 0
                )
            else:
                self.slot(self.at)
            self.at = end

    def pump(self, count=1):
        self.pump_to(self.at + count)

    def finish(self, js):
        self.pump_to(max(self.end(j) for j in js))

    def handed(self, j, whole):
        pltpu.make_async_copy(whole, whole, self.yrecv.at[j]).wait()

    def drain(self, wholes):
        for j, whole in enumerate(wholes):
            for way in (0, 1):
                if self.reach[way] > 0:
                    ref = whole(self.reach[way])
                    pltpu.make_async_copy(ref, ref, self.send_sem.at[j, way]).wait()
            if j in self.shared:
                ref = whole(self.n - 1)
                pltpu.make_async_copy(ref, ref, self.ysend.at[j]).wait()


def layer_kernel(
    n,
    tp,
    tokens,
    mix_gain,
    val_h,
    gate_h,
    conv_taps,
    chan_gain,
    out_h,
    mix_post_gain,
    ffn_gain,
    up_gate_h,
    up_val_h,
    ffn_taps,
    down_h,
    ffn_post_gain,
    out,
    vg,
    outt,
    up,
    downt,
    xg,
    lhs,
    prod,
    din,
    psum,
    opp,
    near,
    comb,
    fin,
    got,
    cbuf,
    conv,
    stats,
    resid,
    fbuf,
    hidden,
    cgain,
    load_sem,
    zsend,
    zrecv,
    ysend,
    yrecv,
    xsend,
    xrecv,
    ssend,
    srecv,
):
    rows, width = tokens.shape
    half, quarter = width // 2, width // 4
    block = width // n
    group_rows = rows * tp
    chip_rows = 2 * rows
    chips = tp // 2
    pieces = up_gate_h.shape[1] // LANES
    f = lax.axis_index("fs")
    t = lax.axis_index("tp")
    x, c = t // 2, lax.rem(t, 2)
    partner = t + 1 - 2 * c
    xr, xl, xo = (lax.rem(x + s, chips) for s in (1, chips - 1, 2))
    tr, tl, to = (2 * v + c for v in (xr, xl, xo))
    odd = c == 1
    g = lax.axis_index("grp")
    side = lax.rem(g, 2)
    mate = g + 1 - 2 * side

    mine = pl.ds(pl.multiple_of(f * block, block), block)
    loads = [
        pltpu.make_async_copy(val_h, vg.at[mine, pl.ds(0, LANES)], load_sem.at[0]),
        pltpu.make_async_copy(gate_h, vg.at[mine, pl.ds(LANES, LANES)], load_sem.at[1]),
    ]
    for j in range(pieces):
        columns = pl.ds(j * LANES, LANES)
        loads.append(
            pltpu.make_async_copy(
                up_gate_h.at[:, columns], up.at[j, mine, pl.ds(0, LANES)], load_sem.at[2 + 2 * j]
            )
        )
        loads.append(
            pltpu.make_async_copy(
                up_val_h.at[:, columns], up.at[j, mine, pl.ds(LANES, LANES)], load_sem.at[3 + 2 * j]
            )
        )
    loads.append(pltpu.make_async_copy(out_h, outt.at[mine, :], load_sem.at[2 + 2 * pieces]))
    loads.append(pltpu.make_async_copy(down_h, downt.at[mine, :], load_sem.at[3 + 2 * pieces]))
    for load in loads:
        load.start()

    barrier = pltpu.get_barrier_semaphore()
    for z in (1, 2, n - 2, n - 1):
        pl.semaphore_signal(barrier, inc=1, device_id={"fs": lax.rem(f + z, n)}, device_id_type=MESH)
    for d in range(1, tp):
        pl.semaphore_signal(
            barrier, inc=1, device_id={"tp": lax.rem(t + d, tp)}, device_id_type=MESH
        )

    pl.semaphore_signal(barrier, inc=1, device_id={"grp": mate}, device_id_type=MESH)

    def zview(buffer, owner):
        return buffer.at[pl.ds(pl.multiple_of(owner * block, block), block), :]

    def down_view(part, owner):
        size = block // 2
        start = pl.multiple_of(owner * block + part * size, size)
        return downt.at[pl.ds(start, size), :]

    share = pieces // 2
    own = [side * share + i for i in range(share)]
    far = [(1 - side) * share + i for i in range(share)]
    both_sides = list(range(2 * share, pieces))
    streams = [functools.partial(zview, vg), functools.partial(zview, outt)]
    streams += [functools.partial(zview, up.at[j]) for j in own]
    streams += [functools.partial(down_view, side)]
    streams += [functools.partial(zview, up.at[j]) for j in both_sides]
    own_at = list(range(2, 2 + share))
    down_at = 2 + share
    both_at = list(range(down_at + 1, len(streams)))
    offsets = [0, min(3, n // 2)] + [0] * share + [min(LATE, n // 2)] * (1 + len(both_sides))
    strides = [2, 2] + [1] * (len(streams) - 2)
    ring = Ring(n, f, streams, offsets, strides, own_at + [down_at], mate, (zsend, zrecv, ysend, yrecv))

    def put_normed(u, left, right, gain):
        scale = lax.rsqrt(
            (
                jnp.sum(left * left, axis=1, keepdims=True)
                + jnp.sum(right * right, axis=1, keepdims=True)
            )
            / width
            + norm_epsilon
        )
        pad = jnp.zeros((8, half), F32)
        for at, part in ((0, left), (half, right)):
            value = part * scale * gain[at : at + half].astype(F32).reshape(1, half)
            low = jnp.concatenate([value, pad], axis=0)
            high = jnp.concatenate([pad, value], axis=0)
            xg[u, t, :, at : at + half] = jnp.where(odd, high, low).astype(BF16)

    def x_copy(u, sem, src, dst, where):
        return pltpu.make_async_remote_copy(
            src_ref=src,
            dst_ref=dst,
            send_sem=xsend.at[u, sem],
            recv_sem=xrecv.at[u, sem],
            device_id={"tp": where},
            device_id_type=MESH,
        )

    first, second = pl.ds(0, half), pl.ds(half, half)

    def spread(u, slots):
        own, from_l, from_r = xg.at[u, t], xg.at[u, tl], xg.at[u, tr]
        opp_l, opp_r = xg.at[u, to, :, first], xg.at[u, to, :, second]
        sent = [
            x_copy(u, 1, own, own, tr),
            x_copy(u, 2, own, own, tl),
            x_copy(u, 0, own, own, partner),
        ]
        for copy in sent:
            copy.start()
        ring.pump_to(slots[0])
        more = []
        x_copy(u, 1, from_l, from_l, tr).wait_recv()
        more.append(x_copy(u, 3, from_l.at[:, first], from_l.at[:, first], tr))
        more.append(x_copy(u, 5, from_l, from_l, partner))
        more[0].start()
        x_copy(u, 2, from_r, from_r, tl).wait_recv()
        more.append(x_copy(u, 4, from_r.at[:, second], from_r.at[:, second], tl))
        more.append(x_copy(u, 6, from_r, from_r, partner))
        for copy in more[2:3] + more[1:2] + more[3:4]:
            copy.start()
        sent += more
        ring.pump_to(slots[1])
        x_copy(u, 3, opp_l, opp_l, tr).wait_recv()
        last = [x_copy(u, 7, opp_l, opp_l, partner)]
        last[0].start()
        x_copy(u, 4, opp_r, opp_r, tl).wait_recv()
        last.append(x_copy(u, 8, opp_r, opp_r, partner))
        last[1].start()
        sent += last
        ring.pump_to(slots[2])
        other = 1 - 2 * c
        for sem, ref in (
            (0, xg.at[u, partner]),
            (5, xg.at[u, tl + other]),
            (6, xg.at[u, tr + other]),
            (7, xg.at[u, to + other, :, first]),
            (8, xg.at[u, to + other, :, second]),
        ):
            x_copy(u, sem, ref, ref, partner).wait_recv()
        for chip in range(chips):
            a, b, base = xg.at[u, 2 * chip], xg.at[u, 2 * chip + 1], chip * chip_rows
            lhs[base : base + 32, :] = a[0:32, :]
            lhs[base + 32 : base + 48, :] = a[32:48, :] + b[0:16, :]
            lhs[base + 48 : base + 80, :] = b[16:48, :]
        return sent

    def chip_rows_at(v):
        return pl.ds(pl.multiple_of(v * chip_rows, 16), chip_rows)

    q0, q1 = pl.ds(0, quarter), pl.ds(quarter, quarter)

    mine_h = pl.ds(pl.multiple_of(c * half, half), half)
    other_h = pl.ds(pl.multiple_of((1 - c) * half, half), half)

    def multiply(u, left, weight, wide):
        sent = x_copy(u, 9, prod.at[u, :, other_h], din.at[u], partner)
        for side_at in (1 - c, c):

            def piece(j, z, side_at=side_at):
                columns = pl.ds(pl.multiple_of(side_at * half + j * wide, wide), wide)
                prod[u, :, columns] = lax.dot_general(
                    left, weight[columns, :], NT, preferred_element_type=F32
                ).astype(BF16)
                return z

            lax.fori_loop(0, half // wide, piece, 0)
            if side_at is not c:
                sent.start()
        return sent

    def collect(u, handed, slots):
        sent = [handed]
        ring.pump_to(slots[0])
        x_copy(u, 9, prod.at[u, :, other_h], din.at[u], partner).wait_recv()
        for v, items in (
            (xo, ((10, q0, opp.at[u, 0], tr), (11, q1, opp.at[u, 1], tl))),
            (xr, ((12, q1, near.at[u, 0, 1], tr),)),
            (xl, ((13, q0, near.at[u, 1, 0], tl),)),
            (x, ()),
        ):
            here = chip_rows_at(v)
            psum[u, here, :] = (
                prod[u, here, mine_h].astype(F32) + din[u, here, :].astype(F32)
            ).astype(BF16)
            for sem, q, dst, where in items:
                copy = x_copy(u, sem, psum.at[u, here, q], dst, where)
                copy.start()
                sent.append(copy)
        ring.pump_to(slots[1])
        for way, sem, v, q, where in ((0, 10, xr, q0, tr), (1, 11, xl, q1, tl)):
            x_copy(u, sem, psum.at[u, chip_rows_at(xo), q], opp.at[u, way], where).wait_recv()
            comb[u, way, :, :] = (
                psum[u, chip_rows_at(v), q].astype(F32) + opp[u, way, :, :].astype(F32)
            ).astype(BF16)
            copy = x_copy(u, 14 + way, comb.at[u, way], near.at[u, way, way], where)
            copy.start()
            sent.append(copy)
        ring.pump_to(slots[2])
        for sem, way, part, where in ((12, 0, 1, tr), (13, 1, 0, tl), (14, 0, 0, tr), (15, 1, 1, tl)):
            x_copy(u, sem, comb.at[u, way], near.at[u, way, part], where).wait_recv()
        for part, q in ((0, q0), (1, q1)):
            fin[u, :, q] = (
                psum[u, chip_rows_at(x), q].astype(F32)
                + near[u, 0, part, :, :].astype(F32)
                + near[u, 1, part, :, :].astype(F32)
            )
        mine_r = pl.ds(pl.multiple_of(c * rows, 8), rows)
        other_r = pl.ds(pl.multiple_of((1 - c) * rows, 8), rows)
        copy = x_copy(u, 16, fin.at[u, other_r, :], got.at[u], partner)
        copy.start()
        sent.append(copy)
        ring.pump_to(slots[3])
        copy.wait_recv()
        here, there = fin[u, mine_r, :], got[u, :, :]
        return jnp.where(odd, there, here), jnp.where(odd, here, there), sent

    left = tokens[:, 0:half].astype(F32)
    right = tokens[:, half:width].astype(F32)
    put_normed(0, left, right, mix_gain)
    cgain[...] = chan_gain[...].astype(F32).reshape(1, -1)
    pl.semaphore_wait(barrier, tp + 4)
    for load in loads:
        load.wait()
    ring.pump_to(1)
    sent = spread(0, (3, 4, 5))

    ring.finish([0])
    ring.pump()
    both = jnp.dot(lhs[...], vg[...], preferred_element_type=F32)
    glu = (both[:, 0:LANES] * jax.nn.sigmoid(both[:, LANES:PAIR])).astype(BF16).astype(F32)
    segments = group_rows // LEN
    taps_n = conv_taps.shape[0]
    cbuf[:, 0:PAD_ROWS, :] = jnp.zeros((segments, PAD_ROWS, LANES), F32)
    for s in range(segments):
        cbuf[s, PAD_ROWS:, :] = glu[s * LEN : (s + 1) * LEN, :]
    my_ch = pl.ds(pl.multiple_of(t * LANES, LANES), LANES)
    taps = conv_taps[:, my_ch].astype(F32)

    def convolve(s, z):
        total = jnp.zeros((LEN, LANES), F32)
        for k in range(taps_n):
            at = PAD_ROWS - (taps_n - 1) + k
            total = total + cbuf[s, at : at + LEN, :] * taps[k : k + 1, :]
        conv[pl.ds(pl.multiple_of(s * LEN, LEN), LEN), :] = total
        return z

    lax.fori_loop(0, segments, convolve, 0)
    conv_out = conv[...]
    ring.pump(1)
    ones = jnp.ones((8, LANES), F32)
    high = lax.Precision.HIGHEST
    sums = lax.dot_general(ones, conv_out, NT, precision=high, preferred_element_type=F32)
    squares = lax.dot_general(
        ones, conv_out * conv_out, NT, precision=high, preferred_element_type=F32
    )
    pick = lax.broadcasted_iota(jnp.int32, (8, group_rows), 0) < 4
    stats[t, :, 0:group_rows] = jnp.where(pick, sums, squares)

    def stat_copy(d):
        return pltpu.make_async_remote_copy(
            src_ref=stats.at[t],
            dst_ref=stats.at[t],
            send_sem=ssend.at[d - 1],
            recv_sem=srecv.at[d - 1],
            device_id={"tp": lax.rem(t + d, tp)},
            device_id_type=MESH,
        )

    stat_copies = [stat_copy(d) for d in range(1, tp)]
    for copy in stat_copies:
        copy.start()
    ring.pump(0)
    for d in range(1, tp):
        source = lax.rem(t + tp - d, tp)
        pltpu.make_async_remote_copy(
            src_ref=stats.at[source],
            dst_ref=stats.at[source],
            send_sem=ssend.at[d - 1],
            recv_sem=srecv.at[d - 1],
            device_id={"tp": source},
            device_id_type=MESH,
        ).wait_recv()
    channels = chan_gain.shape[0]
    both_stats = jnp.sum(stats[:, :, 0:group_rows], axis=0) / channels
    flipped = jnp.transpose(
        jnp.concatenate([both_stats] + [jnp.zeros((8, group_rows), F32)] * 15, axis=0)
    )
    mean, square = flipped[:, 0:1], flipped[:, 4:5]
    scale = lax.rsqrt(square - mean * mean + chan_epsilon)
    normal = (conv_out - mean) * scale * cgain[:, my_ch]
    activated = (normal * jax.nn.sigmoid(normal)).astype(BF16)
    ring.finish([1])
    handed = multiply(0, activated, outt, min(512, half))
    ring.pump(1)
    base = ring.at
    left_sum, right_sum, more = collect(0, handed, (base + 0, base + 1, base + 1, base + 2))
    sent += more

    def rms(a, b, gain):
        scale = lax.rsqrt(
            (jnp.sum(a * a, axis=1, keepdims=True) + jnp.sum(b * b, axis=1, keepdims=True)) / width
            + norm_epsilon
        )
        return (
            a * scale * gain[0:half].astype(F32).reshape(1, half),
            b * scale * gain[half:width].astype(F32).reshape(1, half),
        )

    a, b = rms(left_sum, right_sum, mix_post_gain)
    res_a = (tokens[:, 0:half].astype(F32) + a).astype(BF16)
    res_b = (tokens[:, half:width].astype(F32) + b).astype(BF16)
    resid[:, 0:half] = res_a.astype(F32)
    resid[:, half:width] = res_b.astype(F32)
    put_normed(1, res_a.astype(F32), res_b.astype(F32), ffn_gain)
    base = ring.at
    sent += spread(1, (base + 1, base + 2, base + 2))

    fbuf[:, 0:FPAD, :] = jnp.zeros((segments, FPAD, PAIR), F32)
    ftaps_n = ffn_taps.shape[0]

    def feed(j):
        pair = jnp.dot(lhs[...], up[j], preferred_element_type=F32).astype(BF16).astype(F32)
        for s in range(segments):
            fbuf[s, FPAD:, :] = pair[s * LEN : (s + 1) * LEN, :]
        here = pl.ds(pl.multiple_of(t * (pieces * LANES) + j * LANES, LANES), LANES)
        gate_taps = ffn_taps[:, 0, here].astype(F32)
        val_taps = ffn_taps[:, 1, here].astype(F32)
        for s in range(segments):
            gate = jnp.zeros((LEN, LANES), F32)
            val = jnp.zeros((LEN, LANES), F32)
            for k in range(ftaps_n):
                at = FPAD - (ftaps_n - 1) + k
                gate = gate + fbuf[s, at : at + LEN, 0:LANES] * gate_taps[k : k + 1, :]
                val = val + fbuf[s, at : at + LEN, LANES:PAIR] * val_taps[k : k + 1, :]
            hidden[j, s * LEN : (s + 1) * LEN, :] = (
                jax.nn.gelu(gate, approximate=True) * val
            ).astype(BF16)

    ring.finish(own_at)
    for j in own:
        feed(j)
        ring.pump()
    ring.pump_to(ring.last)
    for j in both_sides:
        feed(j)
    for at, j in zip(own_at, far):
        ring.handed(at, up.at[j, 0 : (n - 1) * block, :])
        feed(j)
    ring.handed(down_at, downt.at[0 : (n - 1) * (block // 2), :])

    units = jnp.concatenate([hidden[i] for i in range(pieces)], axis=1)
    handed = multiply(1, units, downt, min(512, half))
    left_sum, right_sum, more = collect(1, handed, (0, 0, 0, 0))
    sent += more
    a, b = rms(left_sum, right_sum, ffn_post_gain)
    out[:, 0:half] = (resid[:, 0:half] + a).astype(BF16)
    out[:, half:width] = (resid[:, half:width] + b).astype(BF16)

    for copy in sent + stat_copies:
        copy.wait_send()

    def whole_of(buffer, size, count):
        return buffer.at[pl.ds(0, count * size), :]

    wholes = [functools.partial(whole_of, vg, block), functools.partial(whole_of, outt, block)]
    wholes += [functools.partial(whole_of, up.at[0], block)] * share
    wholes += [functools.partial(whole_of, downt, block // 2)]
    wholes += [functools.partial(whole_of, up.at[0], block)] * len(both_sides)
    ring.drain(wholes)


def shards(*args):
    tokens, up_weight = args[0], args[9]
    n, tp = lax.axis_size("fs"), lax.axis_size("tp")
    rows, width = tokens.shape
    half, quarter = width // 2, width // 4
    group_rows, chip_rows = rows * tp, 2 * rows
    segments = group_rows // LEN
    pieces = up_weight.shape[1] // LANES
    streams = 3 + pieces - pieces // 2
    steps = n // 2
    args = list(args)
    args[6], args[12], args[11] = args[6].T, args[12].T, args[11].transpose(1, 0, 2)
    vmem = pl.BlockSpec(memory_space=pltpu.VMEM)
    hbm = pl.BlockSpec(memory_space=pltpu.HBM)
    dma = pltpu.SemaphoreType.DMA
    return pl.pallas_call(
        functools.partial(layer_kernel, n, tp),
        out_shape=jax.ShapeDtypeStruct((rows, width), BF16),
        in_specs=[hbm if i in (2, 3, 6, 9, 10, 12) else vmem for i in range(len(args))],
        out_specs=vmem,
        scratch_shapes=[
            pltpu.VMEM((width, PAIR), BF16),
            pltpu.VMEM((width, LANES), BF16),
            pltpu.VMEM((pieces, width, PAIR), BF16),
            pltpu.VMEM((width, pieces * LANES), BF16),
            pltpu.VMEM((2, tp, rows + 8, width), BF16),
            pltpu.VMEM((group_rows, width), BF16),
            pltpu.VMEM((2, group_rows, width), BF16),
            pltpu.VMEM((2, group_rows, half), BF16),
            pltpu.VMEM((2, group_rows, half), BF16),
            pltpu.VMEM((2, 2, chip_rows, quarter), BF16),
            pltpu.VMEM((2, 2, 2, chip_rows, quarter), BF16),
            pltpu.VMEM((2, 2, chip_rows, quarter), BF16),
            pltpu.VMEM((2, chip_rows, half), F32),
            pltpu.VMEM((2, rows, half), F32),
            pltpu.VMEM((segments, PAD_ROWS + LEN, LANES), F32),
            pltpu.VMEM((group_rows, LANES), F32),
            pltpu.VMEM((tp, 8, pl.cdiv(group_rows, LANES) * LANES), F32),
            pltpu.VMEM((rows, width), F32),
            pltpu.VMEM((segments, FPAD + LEN, PAIR), F32),
            pltpu.VMEM((pieces, group_rows, LANES), BF16),
            pltpu.VMEM((1, args[5].shape[0]), F32),
            dma((4 + 2 * pieces,)),
            dma((streams, 2)),
            dma((streams, 2, steps)),
            dma((streams,)),
            dma((streams,)),
            dma((2, 17)),
            dma((2, 17)),
            dma((tp - 1,)),
            dma((tp - 1,)),
        ],
        compiler_params=pltpu.CompilerParams(
            collective_id=0, has_side_effects=True, vmem_limit_bytes=60 * 1024 * 1024
        ),
    )(*args)


def solution(mesh):
    return jax.shard_map(
        shards,
        mesh=mesh,
        in_specs=(
            P(("grp", "fs", "tp"), None),
            P(),
            P("fs", "tp"),
            P("fs", "tp"),
            P(),
            P(),
            P("tp", "fs"),
            P(),
            P(),
            P("fs", "tp"),
            P("fs", "tp"),
            P(),
            P("tp", "fs"),
            P(),
        ),
        out_specs=P(("grp", "fs", "tp"), None),
        check_vma=False,
    )
```
